256 devices in a mesh: grp: 2 (over y), sp: 32 (over z, core), tp: 4 (over x).
Axes of the slice: x: 4, y: 2, z: 16, core: 2. Of those that a mesh axis runs over, the one named last changes fastest.
The devices are a block of a 4x16x16 slice.
Arguments:
- layer_input: bfloat16 [12288, 2048], P(('grp', 'sp', 'tp')), parts along dimension 0, may hold values from -6 to 6
- latent: bfloat16 [12288, 512], P(('grp', 'sp')), parts along dimension 0, may hold values from -6 to 6
- rope_key: bfloat16 [12288, 64], P(('grp', 'sp')), parts along dimension 0, may hold values from -4 to 4
- query_wide: bfloat16 [12288, 1536], P(('grp', 'sp'), 'tp'), parts along dimension 0, may hold values from -18 to 18
- query_narrow: bfloat16 [12288, 1024], P(('grp', 'sp'), 'tp'), parts along dimension 0, may hold values from -18 to 18
- key_up_wide: bfloat16 [512, 1024], P(None, 'tp'), may hold values from -0.25 to 0.25
- value_up_wide: bfloat16 [512, 1024], P(None, 'tp'), may hold values from -0.25 to 0.25
- key_up_narrow: bfloat16 [512, 512], P(None, 'tp'), may hold values from -0.25 to 0.25
- value_up_narrow: bfloat16 [512, 512], P(None, 'tp'), may hold values from -0.25 to 0.25
- out_wide: bfloat16 [1024, 2048], P('tp'), may hold values from -1.1953125 to 1.1953125
- out_narrow: bfloat16 [512, 2048], P('tp'), may hold values from -1.1953125 to 1.1953125
- norm_gain: float32 [2048], replicated, may hold values from 0.1 to 1.9
- gate_weight: bfloat16 [2048, 5632], P('sp', 'tp'), may hold values from -0.125 to 0.125
- value_weight: bfloat16 [2048, 5632], P('sp', 'tp'), may hold values from -0.125 to 0.125
- conv_weight: float32 [3, 5632], P(None, 'tp'), may hold values from -2.5 to 2.5
- down_weight: bfloat16 [5632, 2048], P('tp', 'sp'), may hold values from -0.078125 to 0.078125
Outputs:
- layer_output: bfloat16 [12288, 2048], P(('grp', 'sp', 'tp')), parts along dimension 0
The draws below stay inside these ranges and needn't reach their ends.
There are 2 independent parts, one for each index of `grp`. The reference program is written for one: setup_inputs(seed, part) draws one part's arguments, and reference() takes and returns one part's arrays. A program takes and returns all parts, laid end to end along the dimension named above; an argument that names none is the same for every part. Nothing has to cross between parts.
All inputs are finite; a program needn't handle non-finite values.
Results may differ from the reference program's by a relative error of at most 0.015.
Values may be sent and summed in bfloat16 or wider, within the bound.
No kernel may reach another device: no remote copies, remote signals or barrier semaphores. Data moves between devices by JAX's collectives and lax.ppermute only.
A program may use at most 128 MiB of HBM per device.

```python
import math
import jax
import jax.numpy as jnp
from jax import lax

D = 2048
LATENT = 512
ROT = 64
NOPE_W = 128
VAL_W = 128
NOPE_N = 64
VAL_N = 64
HEADS_W = 8
HEADS_N = 8
FF = 5632
CONV = 3
TOK_DEV = 192
TOKENS = 6144
N_TP = 4


def planted_rows(key):
    positions = jnp.arange(TOKENS, dtype=jnp.int32)
    planted = jax.random.randint(jax.random.fold_in(key, 101), (TOKENS,), 0, 48) == 0
    offsets = jax.random.randint(jax.random.fold_in(key, 103), (TOKENS,), TOK_DEV, TOKENS - TOK_DEV + 1)
    target = (positions + offsets) % TOKENS
    rotary = jnp.clip(jax.random.normal(jax.random.fold_in(key, 102), (TOKENS, ROT), jnp.float32), -4.0, 4.0)
    return (planted, target, rotary)


def planted_query(key, head_count, nope_width, salt_value):
    planted, target, rotary = planted_rows(key)
    own_key = jax.random.fold_in(key, salt_value)
    drawn = jnp.clip(2.0 * jax.random.normal(own_key, (TOKENS, head_count, nope_width + ROT), jnp.float32), -12.0, 12.0)
    return drawn.reshape(TOKENS, head_count * (nope_width + ROT))


def draw_rope_key(key, part):
    return planted_rows(key)[2].astype(jnp.bfloat16)


def draw_query_wide(key, part):
    return planted_query(key, HEADS_W, NOPE_W, 201).astype(jnp.bfloat16)


def draw_query_narrow(key, part):
    return planted_query(key, HEADS_N, NOPE_N, 202).astype(jnp.bfloat16)


def block_scale(key, dims, shards, least, top_value):
    def one(axis_at, blocks):
        steps = jax.random.uniform(jax.random.fold_in(jax.random.fold_in(key, 6), axis_at), (blocks,), jnp.float32, least / len(shards), top_value / len(shards))
        return jnp.repeat(jnp.exp(steps), dims[axis_at] // blocks).reshape((-1,) + (1,) * (len(dims) - axis_at - 1))

    loudness = one(*shards[0])
    for cut in shards[1:]:
        loudness = loudness * one(*cut)
    return loudness


def centred(stream_key, extent, deviation, bound, cuts=(), kind=jnp.bfloat16):
    values = deviation * jax.random.normal(stream_key, extent, jnp.float32)
    if cuts:
        values = values * block_scale(stream_key, extent, cuts, -0.22, 0.18)
    return jnp.clip(values, -bound, bound).astype(kind)


def setup_inputs(seed: int = 0, part: int = 0) -> dict:
    key_of = jax.random.split(jax.random.key(seed), 17)
    own_keys = jax.random.split(jax.random.fold_in(key_of[16], part), 17)
    return {
        "layer_input": centred(own_keys[0], (TOKENS, D), 1.0, 6.0, ((0, 128),)),
        "latent": centred(own_keys[1], (TOKENS, LATENT), 1.0, 6.0, ((0, 32),)),
        "rope_key": draw_rope_key(jax.random.fold_in(jax.random.fold_in(key_of[16], part), 71), part),
        "query_wide": draw_query_wide(jax.random.fold_in(jax.random.fold_in(key_of[16], part), 71), part),
        "query_narrow": draw_query_narrow(jax.random.fold_in(jax.random.fold_in(key_of[16], part), 71), part),
        "key_up_wide": centred(key_of[5], (LATENT, HEADS_W * NOPE_W), LATENT ** -0.5, 0.25, ((1, 4),)),
        "value_up_wide": centred(key_of[6], (LATENT, HEADS_W * VAL_W), LATENT ** -0.5, 0.25, ((1, 4),)),
        "key_up_narrow": centred(key_of[7], (LATENT, HEADS_N * NOPE_N), LATENT ** -0.5, 0.25, ((1, 4),)),
        "value_up_narrow": centred(key_of[8], (LATENT, HEADS_N * VAL_N), LATENT ** -0.5, 0.25, ((1, 4),)),
        "out_wide": centred(key_of[9], (HEADS_W * VAL_W, D), 0.2, 1.1953125, ((0, 4),)),
        "out_narrow": centred(key_of[10], (HEADS_N * VAL_N, D), 0.2, 1.1953125, ((0, 4),)),
        "norm_gain": jnp.clip(1.0 + 0.18 * jax.random.normal(key_of[11], (D,), jnp.float32), 0.1, 1.9),
        "gate_weight": centred(key_of[12], (D, FF), D ** -0.5, 0.125, ((0, 32), (1, 4))),
        "value_weight": centred(key_of[13], (D, FF), D ** -0.5, 0.125, ((0, 32), (1, 4))),
        "conv_weight": centred(key_of[14], (CONV, FF), 0.6, 2.5, ((1, 4),), jnp.float32),
        "down_weight": centred(key_of[15], (FF, D), FF ** -0.5, 0.078125, ((0, 4), (1, 32))),
    }


rope_base = 10000.0
norm_eps = 1e-06

def rope_tables(row_total, span_width):
    places = jnp.arange(row_total, dtype=jnp.int32).astype(jnp.float32)
    frequency = jnp.power(rope_base, -jnp.arange(0, span_width, 2, dtype=jnp.int32).astype(jnp.float32) / span_width)
    angles = places[:, None] * frequency[None, :]
    angles = jnp.concatenate([angles, angles], axis=-1)
    return (jnp.cos(angles), jnp.sin(angles))

def spin_rows(entries, cosine, sine_table):
    entries = entries.astype(jnp.float32)
    lead_half, tail_half = jnp.split(entries, 2, axis=-1)
    return entries * cosine + jnp.concatenate([-tail_half, lead_half], axis=-1) * sine_table

def group_attention(query, latent, turned_key, key_up, value_up, head_count, nope_width, value_width, cosine, sine_table):
    rot_width = turned_key.shape[1]
    shaped = query.reshape(TOKENS, head_count, nope_width + rot_width)
    nope_q = shaped[:, :, :nope_width]
    rope_q = spin_rows(shaped[:, :, nope_width:], cosine[:, None, :], sine_table[:, None, :]).astype(jnp.bfloat16)
    key_rows = jnp.dot(latent, key_up, preferred_element_type=jnp.float32).astype(jnp.bfloat16)
    key_rows = key_rows.reshape(TOKENS, head_count, nope_width).astype(jnp.float32)
    value_rows = jnp.dot(latent, value_up, preferred_element_type=jnp.float32).astype(jnp.bfloat16)
    value_rows = value_rows.reshape(TOKENS, head_count, value_width).astype(jnp.float32)
    key_turned = turned_key.astype(jnp.float32)
    score_scale = 1.0 / math.sqrt(nope_width + rot_width)

    def one_block(query_block):
        nope_block, rope_block = query_block
        scores = jnp.einsum('qhd,khd->qhk', nope_block.astype(jnp.float32), key_rows)
        scores = (scores + jnp.einsum('qhd,kd->qhk', rope_block.astype(jnp.float32), key_turned)) * score_scale
        weights = jnp.exp(scores - lax.optimization_barrier(jnp.max(scores, axis=-1, keepdims=True)))
        row_sum = lax.optimization_barrier(jnp.sum(weights, axis=-1))
        rounded = lax.optimization_barrier(weights.astype(jnp.bfloat16)).astype(jnp.float32)
        mixed = jnp.einsum('qhk,khd->qhd', rounded, value_rows)
        return (mixed / row_sum[:, :, None]).astype(jnp.bfloat16)
    blocks = TOKENS // TOK_DEV
    nope_blocks = nope_q.reshape(blocks, TOK_DEV, head_count, nope_width)
    rope_blocks = rope_q.reshape(blocks, TOK_DEV, head_count, rot_width)
    result = lax.map(one_block, (nope_blocks, rope_blocks))
    return result.reshape(TOKENS, head_count * value_width)

def reference(layer_input, latent, rope_key, query_wide, query_narrow, key_up_wide, value_up_wide, key_up_narrow, value_up_narrow, out_wide, out_narrow, norm_gain, gate_weight, value_weight, conv_weight, down_weight):
    cosine, sine_table = rope_tables(TOKENS, ROT)
    turned_key = spin_rows(rope_key, cosine, sine_table).astype(jnp.bfloat16)
    wide_att = group_attention(query_wide, latent, turned_key, key_up_wide, value_up_wide, HEADS_W, NOPE_W, VAL_W, cosine, sine_table)
    narrow_att = group_attention(query_narrow, latent, turned_key, key_up_narrow, value_up_narrow, HEADS_N, NOPE_N, VAL_N, cosine, sine_table)
    wide_share = HEADS_W * VAL_W // N_TP
    narrow_share = HEADS_N * VAL_N // N_TP
    head_part = jnp.einsum('tic,icd->itd', wide_att.reshape(TOKENS, N_TP, wide_share).astype(jnp.float32), out_wide.reshape(N_TP, wide_share, D).astype(jnp.float32))
    head_part = head_part + jnp.einsum('tic,icd->itd', narrow_att.reshape(TOKENS, N_TP, narrow_share).astype(jnp.float32), out_narrow.reshape(N_TP, narrow_share, D).astype(jnp.float32))
    head_part = lax.optimization_barrier(head_part.astype(jnp.bfloat16)).astype(jnp.float32)
    middle = (layer_input.astype(jnp.float32) + lax.optimization_barrier(jnp.sum(head_part, axis=0))).astype(jnp.bfloat16)
    middle_full = middle.astype(jnp.float32)
    normed = middle_full * lax.rsqrt(lax.optimization_barrier(jnp.mean(middle_full * middle_full, axis=-1, keepdims=True)) + norm_eps)
    normed = (normed * norm_gain).astype(jnp.bfloat16)
    gate_pre = jnp.dot(normed, gate_weight, preferred_element_type=jnp.float32).astype(jnp.bfloat16)
    value_pre = jnp.dot(normed, value_weight, preferred_element_type=jnp.float32)
    padded = jnp.pad(gate_pre, ((1, 1), (0, 0))).astype(jnp.float32)
    conv_gate = jnp.zeros((TOKENS, FF), jnp.float32)
    for kernel_tap in range(CONV):
        conv_gate = conv_gate + conv_weight[kernel_tap] * padded[kernel_tap:kernel_tap + TOKENS]
    hidden = (jax.nn.silu(conv_gate) * value_pre).astype(jnp.bfloat16)
    hidden_share = FF // N_TP
    channel_part = jnp.einsum('tic,icd->itd', hidden.reshape(TOKENS, N_TP, hidden_share).astype(jnp.float32), down_weight.reshape(N_TP, hidden_share, D).astype(jnp.float32))
    channel_part = lax.optimization_barrier(channel_part.astype(jnp.bfloat16)).astype(jnp.float32)
    return (middle_full + lax.optimization_barrier(jnp.sum(channel_part, axis=0))).astype(jnp.bfloat16)
```

```python
import functools
import math

import jax
import jax.numpy as jnp
from jax import lax
from jax.experimental import pallas as pl
from jax.experimental.pallas import tpu as pltpu
from jax.sharding import PartitionSpec as P

NOPE_W = 128
NOPE_N = 64
CORES = 2
HALO = 16
LOG2E = math.log2(math.e)

rope_base = 10000.0
norm_eps = 1e-06


F32 = jnp.float32
BF16 = jnp.bfloat16
VMEM = pl.BlockSpec(memory_space=pltpu.VMEM)
SMEM = pl.BlockSpec(memory_space=pltpu.SMEM)
ANY = pl.BlockSpec(memory_space=pl.ANY)


def shift_perm(size, by):
    return [(i, (i + by) % size) for i in range(size)]


def partner_perm(size):
    return [(i, i ^ 1) for i in range(size)]


def ring_pieces(own, up_perm, down_perm, length):
    pieces = [(own, 0)]
    up = down = own
    for k in range(1, length // 2 + 1):
        up = lax.ppermute(up, "sp", up_perm)
        pieces.append((up, -k))
        if len(pieces) < length:
            down = lax.ppermute(down, "sp", down_perm)
            pieces.append((down, k))
    return pieces


def dot_nt(a, b):
    return lax.dot_general(a, b, (((1,), (1,)), ((), ())), preferred_element_type=F32)


def dot_nn(a, b):
    return jnp.dot(a, b, preferred_element_type=F32)


def rope_tables(row_start, row_total, span_width):
    places = (row_start + jnp.arange(row_total, dtype=jnp.int32)).astype(F32)
    frequency = jnp.power(
        rope_base, -jnp.arange(0, span_width, 2, dtype=jnp.int32).astype(F32) / span_width
    )
    angles = places[:, None] * frequency[None, :]
    angles = jnp.concatenate([angles, angles], axis=-1)
    return (jnp.cos(angles), jnp.sin(angles))


def prepare_kernel(latent, rope_key, query_wide, query_narrow, cosine, sine, packed, queries):
    cos, sin = cosine[...], sine[...]
    rot = cos.shape[1]

    def spun(entries):
        entries = entries.astype(F32)
        half = rot // 2
        turned = jnp.concatenate([-entries[:, half:], entries[:, :half]], axis=1)
        return (entries * cos + turned * sin).astype(BF16)

    key = spun(rope_key[...])
    width = latent.shape[1]
    packed[:, :width] = latent[...]
    packed[:, width:] = jnp.concatenate([key, key], axis=1)
    blank = jnp.zeros((cos.shape[0], rot), BF16)
    wide = query_wide[...]
    narrow = query_narrow[...]
    size = NOPE_W + rot
    for h in range(2):
        head = wide[:, h * size : (h + 1) * size]
        queries[:, 256 * h : 256 * h + NOPE_W] = head[:, :NOPE_W]
        queries[:, 256 * h + NOPE_W : 256 * h + 256] = jnp.concatenate(
            [spun(head[:, NOPE_W:]), blank], axis=1
        )
    size = NOPE_N + rot
    first, second = narrow[:, :size], narrow[:, size:]
    queries[:, 512:640] = jnp.concatenate([first[:, :NOPE_N], spun(first[:, NOPE_N:])], axis=1)
    queries[:, 640:768] = jnp.concatenate([spun(second[:, NOPE_N:]), second[:, :NOPE_N]], axis=1)


def prepare(latent, rope_key, query_wide, query_narrow, cosine, sine):
    rows = latent.shape[0]
    return pl.pallas_call(
        prepare_kernel,
        out_shape=(
            jax.ShapeDtypeStruct((rows, latent.shape[1] + 128), BF16),
            jax.ShapeDtypeStruct((rows, 768), BF16),
        ),
        in_specs=[VMEM] * 6,
        out_specs=(VMEM, VMEM),
        name="prepare",
    )(latent, rope_key, query_wide, query_narrow, cosine, sine)


def attend_kernel(count, first, scales, *refs):
    q_own, q_other, key_wide, value_wide, key_narrow, value_narrow = refs[:6]
    pieces = refs[6 : 6 + count]
    states = refs[6 + count : 6 + count + (0 if first else 2)]
    own_out, other_out = refs[-2:]
    rows = q_own.shape[0]
    width = key_wide.shape[0]
    latent = jnp.concatenate([p[:, :width] for p in pieces], axis=0)
    turned = jnp.concatenate([p[:, width:] for p in pieces], axis=0)
    wide_keys = dot_nn(latent, key_wide[...]).astype(BF16)
    wide_values = dot_nn(latent, value_wide[...]).astype(BF16)
    narrow_keys = dot_nn(latent, key_narrow[...]).astype(BF16)
    narrow_values = dot_nn(latent, value_narrow[...]).astype(BF16)
    lane = lax.broadcasted_iota(jnp.int32, narrow_keys.shape, 1)
    keys = [
        jnp.concatenate([wide_keys[:, :128], turned], axis=1),
        jnp.concatenate([wide_keys[:, 128:], turned], axis=1),
        jnp.where(lane < NOPE_N, narrow_keys, turned),
        jnp.where(lane < NOPE_N, turned, narrow_keys),
    ]
    values = [wide_values[:, :128], wide_values[:, 128:], narrow_values, narrow_values]
    spans = [(0, 256), (256, 512), (512, 640), (640, 768)]
    out_lane = lax.broadcasted_iota(jnp.int32, (rows, 128), 1)
    for side, (q, out) in enumerate(((q_own, own_out), (q_other, other_out))):
        stats = jnp.zeros((rows, 128), F32)
        narrow_parts = []
        for h in range(4):
            begin, end = spans[h]
            factor = scales[h] * LOG2E
            scores = dot_nt(q[:, begin:end], keys[h])
            top = jnp.max(scores, axis=1, keepdims=True)
            if not first:
                old = states[side]
                old_top = old[:, 384 + h : 385 + h]
                old_sum = old[:, 388 + h : 389 + h]
                top = jnp.maximum(top, old_top)
                shrink = jnp.exp2((old_top - top) * factor)
            prob = jnp.exp2((scores - top) * factor)
            total = jnp.sum(prob, axis=1, keepdims=True)
            mixed = dot_nn(prob.astype(BF16), values[h])
            if not first:
                total = total + old_sum * shrink
                place = min(h, 2) * 128
                mixed = mixed + old[:, place : place + 128] * shrink
            stats = jnp.where(out_lane == h, top, stats)
            stats = jnp.where(out_lane == 4 + h, total, stats)
            if h < 2:
                out[:, h * 128 : h * 128 + 128] = mixed
            else:
                narrow_parts.append(mixed)
        out[:, 256:384] = jnp.where(out_lane < NOPE_N, narrow_parts[0], narrow_parts[1])
        out[:, 384:512] = stats


def attend(q_own, q_other, weights, pieces, states, scales):
    rows = q_own.shape[0]
    keys = sum(p.shape[0] for p in pieces)
    first = states is None
    shape = jax.ShapeDtypeStruct((rows, 512), F32)
    operands = [q_own, q_other, *weights, *pieces, *(() if first else states)]
    return pl.pallas_call(
        functools.partial(attend_kernel, len(pieces), first, scales),
        out_shape=(shape, shape),
        in_specs=[VMEM] * len(operands),
        out_specs=(VMEM, VMEM),
        cost_estimate=pl.CostEstimate(
            flops=2 * keys * (512 * 768 + 2 * rows * 1280),
            bytes_accessed=8 * rows * 512 + 2 * keys * 640 + 2 * 512 * 768,
            transcendentals=8 * rows * keys,
        ),
        name="attend",
    )(*operands)


def project_kernel(parts, scales, index, mine, theirs, out_wide, out_narrow, *refs):
    outs, scratch = refs[:parts], refs[parts]
    rows = mine.shape[0]
    lane = lax.broadcasted_iota(jnp.int32, (rows, 128), 1)
    pieces = []
    for h in range(4):
        factor = scales[h] * LOG2E
        top_a, top_b = mine[:, 384 + h : 385 + h], theirs[:, 384 + h : 385 + h]
        sum_a, sum_b = mine[:, 388 + h : 389 + h], theirs[:, 388 + h : 389 + h]
        top = jnp.maximum(top_a, top_b)
        shrink_a = jnp.exp2((top_a - top) * factor)
        shrink_b = jnp.exp2((top_b - top) * factor)
        total = sum_a * shrink_a + sum_b * shrink_b
        place = min(h, 2) * 128
        mixed = mine[:, place : place + 128] * shrink_a + theirs[:, place : place + 128] * shrink_b
        pieces.append(mixed / total)
    narrow = jnp.where(lane < NOPE_N, pieces[2], pieces[3])
    wide = jnp.concatenate(pieces[:2], axis=1).astype(BF16)
    scratch[...] = dot_nn(wide, out_wide[...]) + dot_nn(narrow.astype(BF16), out_narrow[...])
    share = rows // parts
    for d in range(parts):
        block = lax.rem(index[0] + d, parts)
        start = pl.multiple_of(block * share, 16)
        outs[d][...] = scratch[pl.ds(start, share), :].astype(BF16)


def project(index, mine, theirs, out_wide, out_narrow, parts, scales):
    rows, width = mine.shape[0], out_wide.shape[1]
    shape = jax.ShapeDtypeStruct((rows // parts, width), BF16)
    return pl.pallas_call(
        functools.partial(project_kernel, parts, scales),
        out_shape=(shape,) * parts,
        in_specs=[SMEM] + [VMEM] * 4,
        out_specs=(VMEM,) * parts,
        scratch_shapes=[pltpu.VMEM((rows, width), F32)],
        cost_estimate=pl.CostEstimate(
            flops=2 * rows * width * 384, bytes_accessed=4 * rows * width, transcendentals=0
        ),
        name="project",
    )(index, mine, theirs, out_wide, out_narrow)


def norm_kernel(parts, *refs):
    layer_input, gain = refs[:2]
    terms = refs[2 : 2 + parts]
    middle_out, normed_out = refs[2 + parts :]
    total = terms[0][...].astype(F32)
    for term in terms[1:]:
        total = total + term[...].astype(F32)
    middle = (layer_input[...].astype(F32) + total).astype(BF16)
    middle_out[...] = middle
    full = middle.astype(F32)
    scale = lax.rsqrt(jnp.mean(full * full, axis=1, keepdims=True) + norm_eps)
    normed_out[...] = (full * scale * gain[...]).astype(BF16)


def add_norm(layer_input, gain, terms):
    shape = jax.ShapeDtypeStruct(layer_input.shape, BF16)
    return pl.pallas_call(
        functools.partial(norm_kernel, len(terms)),
        out_shape=(shape, shape),
        in_specs=[VMEM] * (2 + len(terms)),
        out_specs=(VMEM, VMEM),
        name="add_norm",
    )(layer_input, gain, *terms)


def split_kernel(parts, index, mine, theirs, *outs):
    share = mine.shape[0] // parts
    for d in range(parts):
        block = lax.rem(index[0] + d, parts)
        rows = pl.ds(pl.multiple_of(block * share, 16), share)
        outs[d][...] = (mine[rows, :] + theirs[rows, :].astype(F32)).astype(BF16)


def add_split(index, mine, theirs, parts):
    shape = jax.ShapeDtypeStruct((mine.shape[0] // parts, mine.shape[1]), BF16)
    return pl.pallas_call(
        functools.partial(split_kernel, parts),
        out_shape=(shape,) * parts,
        in_specs=[SMEM, VMEM, VMEM],
        out_specs=(VMEM,) * parts,
        name="add_split",
    )(index, mine, theirs)


def finish_kernel(middle, *refs):
    terms, out = refs[:-1], refs[-1]
    total = terms[0][...].astype(F32)
    for term in terms[1:]:
        total = total + term[...].astype(F32)
    out[...] = (middle[...].astype(F32) + total).astype(BF16)


def finish(middle, terms):
    return pl.pallas_call(
        finish_kernel,
        out_shape=jax.ShapeDtypeStruct(middle.shape, BF16),
        in_specs=[VMEM] * (1 + len(terms)),
        out_specs=VMEM,
        name="finish",
    )(middle, *terms)


def mixer_kernel(parts, offsets, index, taps, near, far, *refs):
    count = len(offsets)
    own_blocks, other_blocks = refs[:parts], refs[parts : 2 * parts]
    pieces = refs[2 * parts : 2 * parts + count]
    own_out, other_out = refs[2 * parts + count : 2 * parts + count + 2]
    x, w_gate, w_value, w_down, gate, hidden, sems = refs[2 * parts + count + 2 :]
    units = w_gate.shape[0]
    span = pieces[0].shape[1]
    at_tp, core, at_z = index[0], index[1], index[2]
    copies = []
    for which, target in enumerate((w_gate, w_value, w_down)):
        for j, offset in enumerate(offsets):
            block = lax.rem(at_z + offset + count, count)
            lanes = pl.ds(pl.multiple_of(block * span, span), span)
            copy = pltpu.make_async_copy(
                pieces[j].at[pl.ds(which * units, units), :], target.at[:, lanes], sems.at[which, j]
            )
            copy.start()
            copies.append(copy)
    share = own_blocks[0].shape[0]
    rows = parts * share
    for d in range(parts):
        block = lax.rem(at_tp - d + parts, parts)
        start = pl.multiple_of(HALO + core * rows + block * share, 16)
        x[pl.ds(start, share), :] = own_blocks[d][...]
        start = pl.multiple_of(HALO + (1 - core) * rows + block * share, 16)
        x[pl.ds(start, share), :] = other_blocks[d][...]

    @pl.when(core == 0)
    def _():
        x[:HALO, :] = near[...]
        x[HALO + 2 * rows :, :] = far[...]

    @pl.when(core == 1)
    def _():
        x[:HALO, :] = far[...]
        x[HALO + 2 * rows :, :] = near[...]

    for copy in copies[:count]:
        copy.wait()
    gate[...] = dot_nt(x[...], w_gate[...]).astype(BF16).astype(F32)
    for copy in copies[count : 2 * count]:
        copy.wait()
    value = dot_nt(x[HALO : HALO + 2 * rows, :], w_value[...])
    mixed = taps[0:1, :] * gate[HALO - 1 : HALO - 1 + 2 * rows, :]
    mixed = mixed + taps[1:2, :] * gate[HALO : HALO + 2 * rows, :]
    mixed = mixed + taps[2:3, :] * gate[HALO + 1 : HALO + 1 + 2 * rows, :]
    hidden[...] = (mixed / (1.0 + jnp.exp(-mixed)) * value).astype(BF16)
    for copy in copies[2 * count :]:
        copy.wait()
    start = pl.multiple_of((1 - core) * rows, 16)
    other_out[...] = dot_nn(hidden[pl.ds(start, rows), :], w_down[...]).astype(BF16)
    start = pl.multiple_of(core * rows, 16)
    own_out[...] = dot_nn(hidden[pl.ds(start, rows), :], w_down[...])


def mixer(index, taps, near, far, own_blocks, other_blocks, pieces, offsets):
    parts = len(own_blocks)
    rows = parts * own_blocks[0].shape[0]
    width = own_blocks[0].shape[1]
    units = pieces[0].shape[0] // 3
    count = len(pieces)
    return pl.pallas_call(
        functools.partial(mixer_kernel, parts, offsets),
        out_shape=(
            jax.ShapeDtypeStruct((rows, width), F32),
            jax.ShapeDtypeStruct((rows, width), BF16),
        ),
        in_specs=[SMEM] + [VMEM] * (3 + 2 * parts) + [ANY] * count,
        out_specs=(VMEM, VMEM),
        scratch_shapes=[
            pltpu.VMEM((2 * HALO + 2 * rows, width), BF16),
            pltpu.VMEM((units, width), BF16),
            pltpu.VMEM((units, width), BF16),
            pltpu.VMEM((units, width), BF16),
            pltpu.VMEM((2 * HALO + 2 * rows, units), F32),
            pltpu.VMEM((2 * rows, units), BF16),
            pltpu.SemaphoreType.DMA((3, count)),
        ],
        cost_estimate=pl.CostEstimate(
            flops=12 * rows * width * units,
            bytes_accessed=6 * width * units,
            transcendentals=2 * rows * units,
        ),
        name="mixer",
    )(index, taps, near, far, *own_blocks, *other_blocks, *pieces)


def scattered(blocks, parts):
    return [blocks[0]] + [
        lax.ppermute(blocks[d], "tp", shift_perm(parts, d)) for d in range(1, parts)
    ]


def on_device(
    layer_input,
    latent,
    rope_key,
    query_wide,
    query_narrow,
    key_up_wide,
    value_up_wide,
    key_up_narrow,
    value_up_narrow,
    out_wide,
    out_narrow,
    norm_gain,
    gate_weight,
    value_weight,
    conv_weight,
    down_weight,
):
    n_sp, n_tp = lax.axis_size("sp"), lax.axis_size("tp")
    n_z = n_sp // CORES
    at_sp, at_tp = lax.axis_index("sp"), lax.axis_index("tp")
    core, at_z = at_sp % CORES, at_sp // CORES
    index = jnp.stack([at_tp, core, at_z]).astype(jnp.int32)
    up, down = shift_perm(n_sp, CORES), shift_perm(n_sp, -CORES)
    swap = partner_perm(n_sp)
    rows = latent.shape[0]
    rot = rope_key.shape[1]
    cosine, sine = rope_tables(at_sp * rows, rows, rot)
    wide_scale = 1.0 / math.sqrt(NOPE_W + rot)
    narrow_scale = 1.0 / math.sqrt(NOPE_N + rot)
    scales = (wide_scale, wide_scale, narrow_scale, narrow_scale)

    packed, q_own = prepare(latent, rope_key, query_wide, query_narrow, cosine, sine)
    key_pieces = [p for p, _ in ring_pieces(packed, up, down, n_z)]
    q_other = lax.ppermute(q_own, "sp", swap)

    units = gate_weight.shape[1] // CORES
    stacked = jnp.stack([gate_weight.T, value_weight.T, down_weight])
    keep = lax.dynamic_slice_in_dim(stacked, core * units, units, axis=1)
    give = lax.dynamic_slice_in_dim(stacked, (1 - core) * units, units, axis=1)
    given = lax.ppermute(give, "sp", swap)
    pair = jnp.where(
        core == 0,
        jnp.concatenate([keep, given], axis=2),
        jnp.concatenate([given, keep], axis=2),
    ).reshape(3 * units, -1)
    pair, key_pieces[-1] = lax.optimization_barrier((pair, key_pieces[-1]))
    weight_ring = ring_pieces(pair, up, down, n_z)
    taps = lax.dynamic_slice_in_dim(conv_weight, core * units, units, axis=1)

    weights = (key_up_wide, value_up_wide, key_up_narrow, value_up_narrow)
    cuts = list(range(0, n_z - 4, 4)) + [n_z - 4, n_z - 2, n_z]
    states = None
    for begin, end in zip(cuts, cuts[1:]):
        states = attend(q_own, q_other, weights, key_pieces[begin:end], states, scales)
    theirs = lax.ppermute(states[1], "sp", swap)
    blocks = project(index, states[0], theirs, out_wide, out_narrow, n_tp, scales)
    middle, normed = add_norm(layer_input, norm_gain[None, :], scattered(blocks, n_tp))

    own_blocks = scattered([normed] * n_tp, n_tp)
    other_blocks = [lax.ppermute(b, "sp", swap) for b in own_blocks]
    edge = jnp.where(
        core == 1,
        lax.dynamic_index_in_dim(
            jnp.stack([b[-HALO:] for b in own_blocks]), (at_tp + 1) % n_tp, 0, keepdims=False
        ),
        lax.dynamic_index_in_dim(
            jnp.stack([b[:HALO] for b in own_blocks]), at_tp, 0, keepdims=False
        ),
    )
    across = [(i, i + 1) for i in range(1, n_sp - 1, 2)]
    near = lax.ppermute(edge, "sp", across + [(j, i) for i, j in across])
    far = lax.ppermute(near, "sp", swap)

    offsets = tuple(offset for _, offset in weight_ring)
    mine, other = mixer(
        index, taps, near, far, own_blocks, other_blocks, [p for p, _ in weight_ring], offsets
    )
    theirs = lax.ppermute(other, "sp", swap)
    sums = scattered(add_split(index, mine, theirs, n_tp), n_tp)
    return finish(middle, sums)


def solution(mesh):
    in_specs = (
        P(("grp", "sp", "tp"), None),
        P(("grp", "sp"), None),
        P(("grp", "sp"), None),
        P(("grp", "sp"), "tp"),
        P(("grp", "sp"), "tp"),
        P(None, "tp"),
        P(None, "tp"),
        P(None, "tp"),
        P(None, "tp"),
        P("tp", None),
        P("tp", None),
        P(),
        P("sp", "tp"),
        P("sp", "tp"),
        P(None, "tp"),
        P("tp", "sp"),
    )
    out_specs = P(("grp", "sp", "tp"), None)
    return jax.shard_map(
        on_device, mesh=mesh, in_specs=in_specs, out_specs=out_specs, check_vma=False
    )
```

```python
import functools
import math

import jax
import jax.numpy as jnp
from jax import lax
from jax.experimental import pallas as pl
from jax.experimental.pallas import tpu as pltpu
from jax.sharding import PartitionSpec as P

NOPE_W = 128
NOPE_N = 64
CORES = 2
HALO = 16
LOG2E = math.log2(math.e)

rope_base = 10000.0
norm_eps = 1e-06


F32 = jnp.float32
BF16 = jnp.bfloat16
VMEM = pl.BlockSpec(memory_space=pltpu.VMEM)
SMEM = pl.BlockSpec(memory_space=pltpu.SMEM)
ANY = pl.BlockSpec(memory_space=pl.ANY)


def shift_perm(size, by):
    return [(i, (i + by) % size) for i in range(size)]


def partner_perm(size):
    return [(i, i ^ 1) for i in range(size)]


def dot_nt(a, b):
    return lax.dot_general(a, b, (((1,), (1,)), ((), ())), preferred_element_type=F32)


def dot_nn(a, b):
    return jnp.dot(a, b, preferred_element_type=F32)


def rope_tables(row_start, row_total, span_width):
    places = (row_start + jnp.arange(row_total, dtype=jnp.int32)).astype(F32)
    frequency = jnp.power(
        rope_base, -jnp.arange(0, span_width, 2, dtype=jnp.int32).astype(F32) / span_width
    )
    angles = places[:, None] * frequency[None, :]
    angles = jnp.concatenate([angles, angles], axis=-1)
    return (jnp.cos(angles), jnp.sin(angles))


def prepare_kernel(latent, rope_key, query_wide, query_narrow, cosine, sine, packed, queries):
    cos, sin = cosine[...], sine[...]
    rot = cos.shape[1]

    def spun(entries):
        entries = entries.astype(F32)
        half = rot // 2
        turned = jnp.concatenate([-entries[:, half:], entries[:, :half]], axis=1)
        return (entries * cos + turned * sin).astype(BF16)

    key = spun(rope_key[...])
    width = latent.shape[1]
    packed[:, :width] = latent[...]
    packed[:, width:] = jnp.concatenate([key, key], axis=1)
    blank = jnp.zeros((cos.shape[0], rot), BF16)
    wide = query_wide[...]
    narrow = query_narrow[...]
    size = NOPE_W + rot
    for h in range(2):
        head = wide[:, h * size : (h + 1) * size]
        queries[:, 256 * h : 256 * h + NOPE_W] = head[:, :NOPE_W]
        queries[:, 256 * h + NOPE_W : 256 * h + 256] = jnp.concatenate(
            [spun(head[:, NOPE_W:]), blank], axis=1
        )
    size = NOPE_N + rot
    first, second = narrow[:, :size], narrow[:, size:]
    queries[:, 512:640] = jnp.concatenate([first[:, :NOPE_N], spun(first[:, NOPE_N:])], axis=1)
    queries[:, 640:768] = jnp.concatenate([spun(second[:, NOPE_N:]), second[:, :NOPE_N]], axis=1)


def prepare(latent, rope_key, query_wide, query_narrow, cosine, sine):
    rows = latent.shape[0]
    return pl.pallas_call(
        prepare_kernel,
        out_shape=(
            jax.ShapeDtypeStruct((rows, latent.shape[1] + 128), BF16),
            jax.ShapeDtypeStruct((rows, 768), BF16),
        ),
        in_specs=[VMEM] * 6,
        out_specs=(VMEM, VMEM),
        name="prepare",
    )(latent, rope_key, query_wide, query_narrow, cosine, sine)


def attend_kernel(count, first, scales, *refs):
    queries, key_wide, value_wide, key_narrow, value_narrow = refs[:5]
    pieces = refs[5 : 5 + count]
    old = None if first else refs[5 + count]
    out = refs[-3]
    keys, values = refs[-2:]
    rows = queries.shape[1]
    width = key_wide.shape[0]
    latent = jnp.concatenate([p[:, :width] for p in pieces], axis=0)
    turned = jnp.concatenate([p[:, width:] for p in pieces], axis=0)
    wide_keys = dot_nn(latent, key_wide[...]).astype(BF16)
    narrow_keys = dot_nn(latent, key_narrow[...]).astype(BF16)
    lane = lax.broadcasted_iota(jnp.int32, narrow_keys.shape, 1)
    keys[:, 0:128] = wide_keys[:, :128]
    keys[:, 128:256] = turned
    keys[:, 256:384] = wide_keys[:, 128:]
    keys[:, 384:512] = turned
    keys[:, 512:640] = jnp.where(lane < NOPE_N, narrow_keys, turned)
    keys[:, 640:768] = jnp.where(lane < NOPE_N, turned, narrow_keys)
    values[:, :256] = dot_nn(latent, value_wide[...]).astype(BF16)
    values[:, 256:] = dot_nn(latent, value_narrow[...]).astype(BF16)
    spans = [(0, 256), (256, 512), (512, 640), (640, 768)]
    out_lane = lax.broadcasted_iota(jnp.int32, (rows, 128), 1)

    def one_side(side, carry):
        stats = jnp.zeros((rows, 128), F32)
        narrow_parts = []
        for h in range(4):
            begin, end = spans[h]
            place = min(h, 2) * 128
            factor = scales[h] * LOG2E
            scores = dot_nt(queries[side, :, begin:end], keys[:, begin:end])
            top = jnp.max(scores, axis=1, keepdims=True)
            if not first:
                old_top = old[side, :, 384 + h : 385 + h]
                old_sum = old[side, :, 388 + h : 389 + h]
                top = jnp.maximum(top, old_top)
                shrink = jnp.exp2((old_top - top) * factor)
            prob = jnp.exp2((scores - top) * factor)
            total = jnp.sum(prob, axis=1, keepdims=True)
            mixed = dot_nn(prob.astype(BF16), values[:, place : place + 128])
            if not first:
                total = total + old_sum * shrink
                mixed = mixed + old[side, :, place : place + 128] * shrink
            stats = jnp.where(out_lane == h, top, stats)
            stats = jnp.where(out_lane == 4 + h, total, stats)
            if h < 2:
                out[side, :, place : place + 128] = mixed
            else:
                narrow_parts.append(mixed)
        out[side, :, 256:384] = jnp.where(out_lane < NOPE_N, narrow_parts[0], narrow_parts[1])
        out[side, :, 384:512] = stats
        return carry

    lax.fori_loop(0, queries.shape[0], one_side, 0)


def attend(queries, weights, pieces, state, scales):
    sides, rows = queries.shape[:2]
    keys = sum(p.shape[0] for p in pieces)
    first = state is None
    operands = [queries, *weights, *pieces, *(() if first else (state,))]
    return pl.pallas_call(
        functools.partial(attend_kernel, len(pieces), first, scales),
        out_shape=jax.ShapeDtypeStruct((sides, rows, 512), F32),
        in_specs=[VMEM] * len(operands),
        out_specs=VMEM,
        scratch_shapes=[pltpu.VMEM((keys, 768), BF16), pltpu.VMEM((keys, 384), BF16)],
        cost_estimate=pl.CostEstimate(
            flops=2 * keys * (512 * 768 + 2 * rows * 1280),
            bytes_accessed=8 * rows * 512 + 2 * keys * 640 + 2 * 512 * 768,
            transcendentals=8 * rows * keys,
        ),
        name="attend",
    )(*operands)


def project_kernel(parts, scales, index, mine, theirs, out_wide, out_narrow, *refs):
    outs, scratch = refs[:parts], refs[parts]
    rows = mine.shape[0]
    lane = lax.broadcasted_iota(jnp.int32, (rows, 128), 1)
    pieces = []
    for h in range(4):
        factor = scales[h] * LOG2E
        top_a, top_b = mine[:, 384 + h : 385 + h], theirs[:, 384 + h : 385 + h]
        sum_a, sum_b = mine[:, 388 + h : 389 + h], theirs[:, 388 + h : 389 + h]
        top = jnp.maximum(top_a, top_b)
        shrink_a = jnp.exp2((top_a - top) * factor)
        shrink_b = jnp.exp2((top_b - top) * factor)
        total = sum_a * shrink_a + sum_b * shrink_b
        place = min(h, 2) * 128
        mixed = mine[:, place : place + 128] * shrink_a + theirs[:, place : place + 128] * shrink_b
        pieces.append(mixed / total)
    narrow = jnp.where(lane < NOPE_N, pieces[2], pieces[3])
    wide = jnp.concatenate(pieces[:2], axis=1).astype(BF16)
    scratch[...] = dot_nn(wide, out_wide[...]) + dot_nn(narrow.astype(BF16), out_narrow[...])
    share = rows // parts
    for d in range(parts):
        block = lax.rem(index[0] + d, parts)
        start = pl.multiple_of(block * share, 16)
        outs[d][...] = scratch[pl.ds(start, share), :].astype(BF16)


def project(index, mine, theirs, out_wide, out_narrow, parts, scales):
    rows, width = mine.shape[0], out_wide.shape[1]
    shape = jax.ShapeDtypeStruct((rows // parts, width), BF16)
    return pl.pallas_call(
        functools.partial(project_kernel, parts, scales),
        out_shape=(shape,) * parts,
        in_specs=[SMEM] + [VMEM] * 4,
        out_specs=(VMEM,) * parts,
        scratch_shapes=[pltpu.VMEM((rows, width), F32)],
        cost_estimate=pl.CostEstimate(
            flops=2 * rows * width * 384, bytes_accessed=4 * rows * width, transcendentals=0
        ),
        name="project",
    )(index, mine, theirs, out_wide, out_narrow)


def mixer_kernel(parts, cuts, out_step, index, taps, before, after, *refs):
    blocks, weights = refs[:parts], refs[parts]
    outs = refs[parts + 1 : 2 * parts + 1]
    x, w_gate, w_value, w_down, gate, hidden, terms, sems = refs[2 * parts + 1 :]
    width, units = w_gate.shape
    at_tp = index[0]
    chunks = list(zip(cuts, cuts[1:]))
    copies = []
    for n, (begin, end) in enumerate(chunks):
        for which, target in enumerate((w_gate, w_value)):
            source = weights.at[:, which * units + begin : which * units + end]
            copies.append(
                pltpu.make_async_copy(source, target.at[:, begin:end], sems.at[which, n])
            )
    out_cuts = list(range(0, width, out_step))
    for n, begin in enumerate(out_cuts):
        source = weights.at[begin : begin + out_step, 2 * units :]
        copies.append(
            pltpu.make_async_copy(source, w_down.at[begin : begin + out_step, :], sems.at[2, n])
        )
    for copy in copies:
        copy.start()
    share = blocks[0].shape[0]
    rows = parts * share
    x[:HALO, :] = before[...]
    x[HALO + rows :, :] = after[...]
    for d in range(parts):
        block = lax.rem(at_tp - d + parts, parts)
        start = pl.multiple_of(HALO + block * share, 16)
        x[pl.ds(start, share), :] = blocks[d][...]
    for n, (begin, end) in enumerate(chunks):
        copies[2 * n].wait()
        gate[:, : end - begin] = dot_nn(x[...], w_gate[:, begin:end]).astype(BF16).astype(F32)
        copies[2 * n + 1].wait()
        value = dot_nn(x[HALO : HALO + rows, :], w_value[:, begin:end])
        mixed = jnp.zeros_like(value)
        for tap in range(taps.shape[0]):
            first = HALO - 1 + tap
            mixed = mixed + taps[tap : tap + 1, begin:end] * gate[first : first + rows, : end - begin]
        hidden[:, begin:end] = (mixed / (1.0 + jnp.exp(-mixed)) * value).astype(BF16)
    for n, begin in enumerate(out_cuts):
        copies[2 * len(chunks) + n].wait()
        terms[:, begin : begin + out_step] = dot_nt(hidden[...], w_down[begin : begin + out_step, :])
    for d in range(parts):
        block = lax.rem(at_tp + d, parts)
        start = pl.multiple_of(block * share, 16)
        outs[d][...] = terms[pl.ds(start, share), :].astype(BF16)


def mixer(index, taps, before, after, blocks, weights):
    parts = len(blocks)
    share, width = blocks[0].shape
    rows = parts * share
    units = weights.shape[1] // 3
    cuts = tuple(range(0, units, 384)) + (units,)
    out_step = width // 4
    return pl.pallas_call(
        functools.partial(mixer_kernel, parts, cuts, out_step),
        out_shape=(jax.ShapeDtypeStruct((share, width), BF16),) * parts,
        in_specs=[SMEM] + [VMEM] * (3 + parts) + [ANY],
        out_specs=(VMEM,) * parts,
        scratch_shapes=[
            pltpu.VMEM((2 * HALO + rows, width), BF16),
            pltpu.VMEM((width, units), BF16),
            pltpu.VMEM((width, units), BF16),
            pltpu.VMEM((width, units), BF16),
            pltpu.VMEM((2 * HALO + rows, 384), F32),
            pltpu.VMEM((rows, units), BF16),
            pltpu.VMEM((rows, width), F32),
            pltpu.SemaphoreType.DMA((3, max(len(cuts) - 1, 4))),
        ],
        cost_estimate=pl.CostEstimate(
            flops=6 * rows * width * units,
            bytes_accessed=6 * width * units,
            transcendentals=rows * units,
        ),
        name="mixer",
    )(index, taps, before, after, *blocks, weights)


def fence(live):
    names = list(live)
    return dict(zip(names, lax.optimization_barrier(tuple(live[n] for n in names))))


def on_device(
    layer_input,
    latent,
    rope_key,
    query_wide,
    query_narrow,
    key_up_wide,
    value_up_wide,
    key_up_narrow,
    value_up_narrow,
    out_wide,
    out_narrow,
    norm_gain,
    gate_weight,
    value_weight,
    conv_weight,
    down_weight,
):
    n_sp, n_tp = lax.axis_size("sp"), lax.axis_size("tp")
    n_z = n_sp // CORES
    steps = {"up": n_z // 2, "down": n_z - 1 - n_z // 2}
    at_sp, at_tp = lax.axis_index("sp"), lax.axis_index("tp")
    index = at_tp.astype(jnp.int32)[None]
    z_moves = {"up": shift_perm(n_sp, CORES), "down": shift_perm(n_sp, -CORES)}
    x_moves = {"up": shift_perm(n_tp, 1), "down": shift_perm(n_tp, -1)}
    swap = partner_perm(n_sp)
    rows = latent.shape[0]
    rot = rope_key.shape[1]
    wide_scale = 1.0 / math.sqrt(NOPE_W + rot)
    narrow_scale = 1.0 / math.sqrt(NOPE_N + rot)
    scales = (wide_scale, wide_scale, narrow_scale, narrow_scale)
    up_weights = (key_up_wide, value_up_wide, key_up_narrow, value_up_narrow)

    stacked = jnp.concatenate([gate_weight, value_weight, down_weight.T], axis=1)
    weights = lax.all_gather(stacked, "sp", axis=0, tiled=True)

    cosine, sine = rope_tables(at_sp * rows, rows, rot)
    packed, q_own = prepare(latent, rope_key, query_wide, query_narrow, cosine, sine)
    half = lax.dynamic_slice_in_dim(packed, (at_tp % 2) * (rows // 2), rows // 2, axis=0)
    live = {"up": half, "down": half, "q": q_own}
    arrived = [packed]
    batch = {"up": [], "down": []}
    state = None
    last = steps["up"]
    for tick in range(1, last + 2):
        new = {}
        for way in ("up", "down"):
            if tick <= steps[way]:
                new[way] = lax.ppermute(live[way], "sp", z_moves[way])
            held = [n for n in live if n.startswith("hold" + way)]
            if held and (len(held) == 2 or tick == last + 1):
                pieces = [live.pop(n) for n in held]
                joined = pieces[0] if len(pieces) == 1 else jnp.concatenate(pieces, axis=0)
                new["x" + way] = lax.ppermute(joined, "tp", x_moves[way])
        if tick == 1:
            new["q"] = jnp.stack([live["q"], lax.ppermute(live["q"], "sp", swap)])
        elif sum(p.shape[0] for p in arrived) >= 2 * rows or tick > last:
            state = attend(live["q"], up_weights, arrived, state, scales)
            arrived = []
            new["state"] = state
        for name in live:
            if name not in new and (name in ("q", "state") or name.startswith("hold")):
                new[name] = live[name]
        live = fence(new)
        state = live.get("state")
        for way in ("up", "down"):
            if tick <= steps[way]:
                arrived.append(live[way])
                live[f"hold{way}{tick}"] = live[way]
            if "x" + way in live:
                arrived.append(live["x" + way])
    state = attend(live["q"], up_weights, arrived, state, scales)
    theirs = lax.ppermute(state[1], "sp", swap)
    blocks = project(index, state[0], theirs, out_wide, out_narrow, n_tp, scales)

    total = blocks[0].astype(F32)
    for d in range(1, n_tp):
        total = total + lax.ppermute(blocks[d], "tp", shift_perm(n_tp, d)).astype(F32)
    middle = (layer_input.astype(F32) + total).astype(BF16)
    full = middle.astype(F32)
    scale = lax.rsqrt(jnp.mean(full * full, axis=-1, keepdims=True) + norm_eps)
    normed = (full * scale * norm_gain).astype(BF16)
    blocks = [normed] + [
        lax.ppermute(normed, "tp", shift_perm(n_tp, d)) for d in range(1, n_tp)
    ]
    tails = jnp.stack([b[-HALO:] for b in blocks])
    heads = jnp.stack([b[:HALO] for b in blocks])
    tail = lax.dynamic_index_in_dim(tails, (at_tp + 1) % n_tp, 0, False)
    head = lax.dynamic_index_in_dim(heads, at_tp, 0, False)
    forward = [(i, i + 1) for i in range(n_sp - 1)]
    before = lax.ppermute(tail, "sp", forward)
    after = lax.ppermute(head, "sp", [(j, i) for i, j in forward])
    blocks, before, after, weights = lax.optimization_barrier((blocks, before, after, weights))
    terms = mixer(index, conv_weight, before, after, blocks, weights)
    total = terms[0].astype(F32)
    for d in range(1, n_tp):
        total = total + lax.ppermute(terms[d], "tp", shift_perm(n_tp, d)).astype(F32)
    return (middle.astype(F32) + total).astype(BF16)


def solution(mesh):
    in_specs = (
        P(("grp", "sp", "tp"), None),
        P(("grp", "sp"), None),
        P(("grp", "sp"), None),
        P(("grp", "sp"), "tp"),
        P(("grp", "sp"), "tp"),
        P(None, "tp"),
        P(None, "tp"),
        P(None, "tp"),
        P(None, "tp"),
        P("tp", None),
        P("tp", None),
        P(),
        P("sp", "tp"),
        P("sp", "tp"),
        P(None, "tp"),
        P("tp", "sp"),
    )
    out_specs = P(("grp", "sp", "tp"), None)
    return jax.shard_map(
        on_device, mesh=mesh, in_specs=in_specs, out_specs=out_specs, check_vma=False
    )
```

```python
import functools
import math

import jax
import jax.numpy as jnp
from jax import lax
from jax.experimental import pallas as pl
from jax.experimental.pallas import tpu as pltpu
from jax.sharding import PartitionSpec as P

NOPE_W = 128
NOPE_N = 64
CORES = 2
HALO = 16
LOG2E = math.log2(math.e)

rope_base = 10000.0
norm_eps = 1e-06


F32 = jnp.float32
BF16 = jnp.bfloat16
VMEM = pl.BlockSpec(memory_space=pltpu.VMEM)
SMEM = pl.BlockSpec(memory_space=pltpu.SMEM)
ANY = pl.BlockSpec(memory_space=pl.ANY)


def shift_perm(size, by):
    return [(i, (i + by) % size) for i in range(size)]


def partner_perm(size):
    return [(i, i ^ 1) for i in range(size)]


def dot_nt(a, b):
    return lax.dot_general(a, b, (((1,), (1,)), ((), ())), preferred_element_type=F32)


def dot_nn(a, b):
    return jnp.dot(a, b, preferred_element_type=F32)


def rope_tables(row_start, row_total, span_width):
    places = (row_start + jnp.arange(row_total, dtype=jnp.int32)).astype(F32)
    frequency = jnp.power(
        rope_base, -jnp.arange(0, span_width, 2, dtype=jnp.int32).astype(F32) / span_width
    )
    angles = places[:, None] * frequency[None, :]
    angles = jnp.concatenate([angles, angles], axis=-1)
    return (jnp.cos(angles), jnp.sin(angles))


def prepare_kernel(
    index, latent, rope_key, query_wide, query_narrow, cosine, sine, packed, half, queries
):
    cos, sin = cosine[...], sine[...]
    rot = cos.shape[1]

    def spun(entries):
        entries = entries.astype(F32)
        half = rot // 2
        turned = jnp.concatenate([-entries[:, half:], entries[:, :half]], axis=1)
        return (entries * cos + turned * sin).astype(BF16)

    key = spun(rope_key[...])
    width = latent.shape[1]
    packed[:, :width] = latent[...]
    packed[:, width:] = jnp.concatenate([key, key], axis=1)
    share = half.shape[0]
    half[...] = packed[pl.ds(pl.multiple_of(lax.rem(index[0], 2) * share, 16), share), :]
    blank = jnp.zeros((cos.shape[0], rot), BF16)
    wide = query_wide[...]
    narrow = query_narrow[...]
    size = NOPE_W + rot
    for h in range(2):
        head = wide[:, h * size : (h + 1) * size]
        queries[:, 256 * h : 256 * h + NOPE_W] = head[:, :NOPE_W]
        queries[:, 256 * h + NOPE_W : 256 * h + 256] = jnp.concatenate(
            [spun(head[:, NOPE_W:]), blank], axis=1
        )
    size = NOPE_N + rot
    first, second = narrow[:, :size], narrow[:, size:]
    queries[:, 512:640] = jnp.concatenate([first[:, :NOPE_N], spun(first[:, NOPE_N:])], axis=1)
    queries[:, 640:768] = jnp.concatenate([spun(second[:, NOPE_N:]), second[:, :NOPE_N]], axis=1)


def prepare(index, latent, rope_key, query_wide, query_narrow, cosine, sine):
    rows = latent.shape[0]
    return pl.pallas_call(
        prepare_kernel,
        out_shape=(
            jax.ShapeDtypeStruct((rows, latent.shape[1] + 128), BF16),
            jax.ShapeDtypeStruct((rows // 2, latent.shape[1] + 128), BF16),
            jax.ShapeDtypeStruct((rows, 768), BF16),
        ),
        in_specs=[SMEM] + [VMEM] * 6,
        out_specs=(VMEM,) * 3,
        name="prepare",
    )(index, latent, rope_key, query_wide, query_narrow, cosine, sine)


def attend_kernel(count, first, last, scales, *refs):
    q_own, q_other, key_wide, value_wide, key_narrow, value_narrow = refs[:6]
    pieces = refs[6 : 6 + count]
    old = None if first else refs[6 + count]
    outs = refs[-4 if last else -3 : -2]
    keys, values = refs[-2:]
    rows = q_own.shape[0]
    width = key_wide.shape[0]
    latent = jnp.concatenate([p[:, :width] for p in pieces], axis=0)
    turned = jnp.concatenate([p[:, width:] for p in pieces], axis=0)
    wide_keys = dot_nn(latent, key_wide[...]).astype(BF16)
    narrow_keys = dot_nn(latent, key_narrow[...]).astype(BF16)
    lane = lax.broadcasted_iota(jnp.int32, narrow_keys.shape, 1)
    keys[:, 0:128] = wide_keys[:, :128]
    keys[:, 128:256] = turned
    keys[:, 256:384] = wide_keys[:, 128:]
    keys[:, 384:512] = turned
    keys[:, 512:640] = jnp.where(lane < NOPE_N, narrow_keys, turned)
    keys[:, 640:768] = jnp.where(lane < NOPE_N, turned, narrow_keys)
    values[:, :256] = dot_nn(latent, value_wide[...]).astype(BF16)
    values[:, 256:] = dot_nn(latent, value_narrow[...]).astype(BF16)
    spans = [(0, 256), (256, 512), (512, 640), (640, 768)]
    out_lane = lax.broadcasted_iota(jnp.int32, (2 * rows, 128), 1)

    def put(begin, end, value):
        if last:
            outs[0][:, begin:end] = value[:rows]
            outs[1][:, begin:end] = value[rows:]
        else:
            outs[0][:, begin:end] = value

    stats = jnp.zeros((2 * rows, 128), F32)
    narrow_parts = []
    for h in range(4):
        begin, end = spans[h]
        place = min(h, 2) * 128
        factor = scales[h] * LOG2E
        q = jnp.concatenate([q_own[:, begin:end], q_other[:, begin:end]], axis=0)
        scores = dot_nt(q, keys[:, begin:end])
        top = jnp.max(scores, axis=1, keepdims=True)
        if not first:
            old_top = old[:, 384 + h : 385 + h]
            old_sum = old[:, 388 + h : 389 + h]
            top = jnp.maximum(top, old_top)
            shrink = jnp.exp2((old_top - top) * factor)
        prob = jnp.exp2((scores - top) * factor)
        total = jnp.sum(prob, axis=1, keepdims=True)
        mixed = dot_nn(prob.astype(BF16), values[:, place : place + 128])
        if not first:
            total = total + old_sum * shrink
            mixed = mixed + old[:, place : place + 128] * shrink
        stats = jnp.where(out_lane == h, top, stats)
        stats = jnp.where(out_lane == 4 + h, total, stats)
        if h < 2:
            put(place, place + 128, mixed)
        else:
            narrow_parts.append(mixed)
    put(256, 384, jnp.where(out_lane < NOPE_N, narrow_parts[0], narrow_parts[1]))
    put(384, 512, stats)


def attend(queries, weights, pieces, state, scales, last=False):
    rows = queries[0].shape[0]
    keys = sum(p.shape[0] for p in pieces)
    first = state is None
    operands = [*queries, *weights, *pieces, *(() if first else (state,))]
    side = jax.ShapeDtypeStruct((rows, 512), F32)
    both = jax.ShapeDtypeStruct((2 * rows, 512), F32)
    return pl.pallas_call(
        functools.partial(attend_kernel, len(pieces), first, last, scales),
        out_shape=(side, side) if last else both,
        in_specs=[VMEM] * len(operands),
        out_specs=(VMEM, VMEM) if last else VMEM,
        scratch_shapes=[pltpu.VMEM((keys, 768), BF16), pltpu.VMEM((keys, 384), BF16)],
        cost_estimate=pl.CostEstimate(
            flops=2 * keys * (512 * 768 + 2 * rows * 1280),
            bytes_accessed=8 * rows * 512 + 2 * keys * 640 + 2 * 512 * 768,
            transcendentals=8 * rows * keys,
        ),
        name="attend",
    )(*operands)


def project_kernel(parts, scales, index, mine, theirs, out_wide, out_narrow, *refs):
    outs, scratch = refs[:parts], refs[parts]
    rows = mine.shape[0]
    lane = lax.broadcasted_iota(jnp.int32, (rows, 128), 1)
    pieces = []
    for h in range(4):
        factor = scales[h] * LOG2E
        top_a, top_b = mine[:, 384 + h : 385 + h], theirs[:, 384 + h : 385 + h]
        sum_a, sum_b = mine[:, 388 + h : 389 + h], theirs[:, 388 + h : 389 + h]
        top = jnp.maximum(top_a, top_b)
        shrink_a = jnp.exp2((top_a - top) * factor)
        shrink_b = jnp.exp2((top_b - top) * factor)
        total = sum_a * shrink_a + sum_b * shrink_b
        place = min(h, 2) * 128
        mixed = mine[:, place : place + 128] * shrink_a + theirs[:, place : place + 128] * shrink_b
        pieces.append(mixed / total)
    narrow = jnp.where(lane < NOPE_N, pieces[2], pieces[3])
    wide = jnp.concatenate(pieces[:2], axis=1).astype(BF16)
    scratch[...] = dot_nn(wide, out_wide[...]) + dot_nn(narrow.astype(BF16), out_narrow[...])
    share = rows // parts
    for d in range(parts):
        block = lax.rem(index[0] + d, parts)
        start = pl.multiple_of(block * share, 16)
        outs[d][...] = scratch[pl.ds(start, share), :].astype(BF16)


def project(index, mine, theirs, out_wide, out_narrow, parts, scales):
    rows, width = mine.shape[0], out_wide.shape[1]
    shape = jax.ShapeDtypeStruct((rows // parts, width), BF16)
    return pl.pallas_call(
        functools.partial(project_kernel, parts, scales),
        out_shape=(shape,) * parts,
        in_specs=[SMEM] + [VMEM] * 4,
        out_specs=(VMEM,) * parts,
        scratch_shapes=[pltpu.VMEM((rows, width), F32)],
        cost_estimate=pl.CostEstimate(
            flops=2 * rows * width * 384, bytes_accessed=4 * rows * width, transcendentals=0
        ),
        name="project",
    )(index, mine, theirs, out_wide, out_narrow)


def mixer_kernel(parts, cuts, out_step, index, taps, before, after, *refs):
    blocks, weights = refs[:parts], refs[parts]
    outs = refs[parts + 1 : 2 * parts + 1]
    x, w_gate, w_value, w_down, gate, hidden, terms, sems = refs[2 * parts + 1 :]
    width, units = w_gate.shape
    at_tp = index[0]
    chunks = list(zip(cuts, cuts[1:]))
    copies = []
    for n, (begin, end) in enumerate(chunks):
        for which, target in enumerate((w_gate, w_value)):
            source = weights.at[:, which * units + begin : which * units + end]
            copies.append(
                pltpu.make_async_copy(source, target.at[:, begin:end], sems.at[which, n])
            )
    out_cuts = list(range(0, width, out_step))
    for n, begin in enumerate(out_cuts):
        source = weights.at[begin : begin + out_step, 2 * units :]
        copies.append(
            pltpu.make_async_copy(source, w_down.at[begin : begin + out_step, :], sems.at[2, n])
        )
    for copy in copies:
        copy.start()
    share = blocks[0].shape[0]
    rows = parts * share
    x[:HALO, :] = before[...]
    x[HALO + rows :, :] = after[...]
    for d in range(parts):
        block = lax.rem(at_tp - d + parts, parts)
        start = pl.multiple_of(HALO + block * share, 16)
        x[pl.ds(start, share), :] = blocks[d][...]
    for n, (begin, end) in enumerate(chunks):
        copies[2 * n].wait()
        gate[:, : end - begin] = dot_nn(x[...], w_gate[:, begin:end]).astype(BF16).astype(F32)
        copies[2 * n + 1].wait()
        value = dot_nn(x[HALO : HALO + rows, :], w_value[:, begin:end])
        mixed = jnp.zeros_like(value)
        for tap in range(taps.shape[0]):
            first = HALO - 1 + tap
            mixed = mixed + taps[tap : tap + 1, begin:end] * gate[first : first + rows, : end - begin]
        hidden[:, begin:end] = (mixed / (1.0 + jnp.exp(-mixed)) * value).astype(BF16)
    for n, begin in enumerate(out_cuts):
        copies[2 * len(chunks) + n].wait()
        terms[:, begin : begin + out_step] = dot_nt(hidden[...], w_down[begin : begin + out_step, :])
    for d in range(parts):
        block = lax.rem(at_tp + d, parts)
        start = pl.multiple_of(block * share, 16)
        outs[d][...] = terms[pl.ds(start, share), :].astype(BF16)


def mixer(index, taps, before, after, blocks, weights):
    parts = len(blocks)
    share, width = blocks[0].shape
    rows = parts * share
    units = weights.shape[1] // 3
    cuts = tuple(range(0, units, 384)) + (units,)
    out_step = width // 4
    return pl.pallas_call(
        functools.partial(mixer_kernel, parts, cuts, out_step),
        out_shape=(jax.ShapeDtypeStruct((share, width), BF16),) * parts,
        in_specs=[SMEM] + [VMEM] * (3 + parts) + [ANY],
        out_specs=(VMEM,) * parts,
        scratch_shapes=[
            pltpu.VMEM((2 * HALO + rows, width), BF16),
            pltpu.VMEM((width, units), BF16),
            pltpu.VMEM((width, units), BF16),
            pltpu.VMEM((width, units), BF16),
            pltpu.VMEM((2 * HALO + rows, 384), F32),
            pltpu.VMEM((rows, units), BF16),
            pltpu.VMEM((rows, width), F32),
            pltpu.SemaphoreType.DMA((3, max(len(cuts) - 1, 4))),
        ],
        cost_estimate=pl.CostEstimate(
            flops=6 * rows * width * units,
            bytes_accessed=6 * width * units,
            transcendentals=rows * units,
        ),
        name="mixer",
    )(index, taps, before, after, *blocks, weights)


def fence(live):
    names = list(live)
    return dict(zip(names, lax.optimization_barrier(tuple(live[n] for n in names))))


def on_device(
    layer_input,
    latent,
    rope_key,
    query_wide,
    query_narrow,
    key_up_wide,
    value_up_wide,
    key_up_narrow,
    value_up_narrow,
    out_wide,
    out_narrow,
    norm_gain,
    gate_weight,
    value_weight,
    conv_weight,
    down_weight,
):
    n_sp, n_tp = lax.axis_size("sp"), lax.axis_size("tp")
    n_z = n_sp // CORES
    steps = {"up": n_z // 2, "down": n_z - 1 - n_z // 2}
    at_sp, at_tp = lax.axis_index("sp"), lax.axis_index("tp")
    index = at_tp.astype(jnp.int32)[None]
    z_moves = {"up": shift_perm(n_sp, CORES), "down": shift_perm(n_sp, -CORES)}
    x_moves = {"up": shift_perm(n_tp, 1), "down": shift_perm(n_tp, -1)}
    swap = partner_perm(n_sp)
    rows = latent.shape[0]
    rot = rope_key.shape[1]
    wide_scale = 1.0 / math.sqrt(NOPE_W + rot)
    narrow_scale = 1.0 / math.sqrt(NOPE_N + rot)
    scales = (wide_scale, wide_scale, narrow_scale, narrow_scale)
    up_weights = (key_up_wide, value_up_wide, key_up_narrow, value_up_narrow)

    stacked = jnp.concatenate([gate_weight, value_weight, down_weight.T], axis=1)
    weights = lax.all_gather(stacked, "sp", axis=0, tiled=True)

    cosine, sine = rope_tables(at_sp * rows, rows, rot)
    packed, half, q_own = prepare(
        index, latent, rope_key, query_wide, query_narrow, cosine, sine
    )
    live = {"up": half, "down": half, "q": q_own}
    arrived, held = [packed], {"up": [], "down": []}
    state = None
    last = steps["up"]
    batch_ticks = (last // 2 + 1, last + 1)
    for tick in range(1, last + 2):
        new = {}
        if tick in batch_ticks:
            for way in ("up", "down"):
                pieces = [live[n] for n in held[way]]
                if not pieces:
                    continue
                joined = pieces[0] if len(pieces) == 1 else jnp.concatenate(pieces, axis=0)
                new["x" + way] = lax.ppermute(joined, "tp", x_moves[way])
        for way in ("up", "down"):
            if tick <= steps[way]:
                new[way] = lax.ppermute(live[way], "sp", z_moves[way])
        if tick == 1:
            new["q_other"] = lax.ppermute(live["q"], "sp", swap)
        if tick in batch_ticks:
            queries = (live["q"], live["q_other"])
            new["state"] = attend(queries, up_weights, arrived, state, scales)
            arrived, held = [], {"up": [], "down": []}
        for name in live:
            if name not in new and (name in ("q", "q_other") or name in held["up"] + held["down"]):
                new[name] = live[name]
        live = fence(new)
        state = live.get("state", state)
        for way in ("up", "down"):
            if tick <= steps[way]:
                arrived.append(live[way])
                held[way].append(f"{way}{tick}")
                live[f"{way}{tick}"] = live[way]
            if "x" + way in live:
                arrived.append(live["x" + way])
    queries = (live["q"], live["q_other"])
    state = attend(queries, up_weights, arrived, state, scales, last=True)
    theirs = lax.ppermute(state[1], "sp", swap)
    blocks = project(index, state[0], theirs, out_wide, out_narrow, n_tp, scales)

    total = blocks[0].astype(F32)
    for d in range(1, n_tp):
        total = total + lax.ppermute(blocks[d], "tp", shift_perm(n_tp, d)).astype(F32)
    middle = (layer_input.astype(F32) + total).astype(BF16)
    full = middle.astype(F32)
    scale = lax.rsqrt(jnp.mean(full * full, axis=-1, keepdims=True) + norm_eps)
    normed = (full * scale * norm_gain).astype(BF16)
    blocks = [normed] + [
        lax.ppermute(normed, "tp", shift_perm(n_tp, d)) for d in range(1, n_tp)
    ]
    tails = jnp.stack([b[-HALO:] for b in blocks])
    heads = jnp.stack([b[:HALO] for b in blocks])
    tail = lax.dynamic_index_in_dim(tails, (at_tp + 1) % n_tp, 0, False)
    head = lax.dynamic_index_in_dim(heads, at_tp, 0, False)
    forward = [(i, i + 1) for i in range(n_sp - 1)]
    before = lax.ppermute(tail, "sp", forward)
    after = lax.ppermute(head, "sp", [(j, i) for i, j in forward])
    blocks, before, after, weights = lax.optimization_barrier((blocks, before, after, weights))
    terms = mixer(index, conv_weight, before, after, blocks, weights)
    total = terms[0].astype(F32)
    for d in range(1, n_tp):
        total = total + lax.ppermute(terms[d], "tp", shift_perm(n_tp, d)).astype(F32)
    return (middle.astype(F32) + total).astype(BF16)


def solution(mesh):
    in_specs = (
        P(("grp", "sp", "tp"), None),
        P(("grp", "sp"), None),
        P(("grp", "sp"), None),
        P(("grp", "sp"), "tp"),
        P(("grp", "sp"), "tp"),
        P(None, "tp"),
        P(None, "tp"),
        P(None, "tp"),
        P(None, "tp"),
        P("tp", None),
        P("tp", None),
        P(),
        P("sp", "tp"),
        P("sp", "tp"),
        P(None, "tp"),
        P("tp", "sp"),
    )
    out_specs = P(("grp", "sp", "tp"), None)
    return jax.shard_map(
        on_device, mesh=mesh, in_specs=in_specs, out_specs=out_specs, check_vma=False
    )
```

```python
import functools
import math

import jax
import jax.numpy as jnp
from jax import lax
from jax.experimental import pallas as pl
from jax.experimental.pallas import tpu as pltpu
from jax.sharding import PartitionSpec as P

NOPE_W = 128
NOPE_N = 64
CORES = 2
HALO = 16
GATHER_AFTER = 3
LOG2E = math.log2(math.e)

rope_base = 10000.0
norm_eps = 1e-06


F32 = jnp.float32
BF16 = jnp.bfloat16
VMEM = pl.BlockSpec(memory_space=pltpu.VMEM)
SMEM = pl.BlockSpec(memory_space=pltpu.SMEM)
ANY = pl.BlockSpec(memory_space=pl.ANY)


def shift_perm(size, by):
    return [(i, (i + by) % size) for i in range(size)]


def partner_perm(size):
    return [(i, i ^ 1) for i in range(size)]


def dot_nt(a, b):
    return lax.dot_general(a, b, (((1,), (1,)), ((), ())), preferred_element_type=F32)


def dot_nn(a, b):
    return jnp.dot(a, b, preferred_element_type=F32)


def rope_tables(row_start, row_total, span_width):
    places = (row_start + jnp.arange(row_total, dtype=jnp.int32)).astype(F32)
    frequency = jnp.power(
        rope_base, -jnp.arange(0, span_width, 2, dtype=jnp.int32).astype(F32) / span_width
    )
    angles = places[:, None] * frequency[None, :]
    angles = jnp.concatenate([angles, angles], axis=-1)
    return (jnp.cos(angles), jnp.sin(angles))


def prepare_kernel(
    index, latent, rope_key, query_wide, query_narrow, cosine, sine, packed, half, queries
):
    cos, sin = cosine[...], sine[...]
    rot = cos.shape[1]

    def spun(entries):
        entries = entries.astype(F32)
        half = rot // 2
        turned = jnp.concatenate([-entries[:, half:], entries[:, :half]], axis=1)
        return (entries * cos + turned * sin).astype(BF16)

    key = spun(rope_key[...])
    width = latent.shape[1]
    packed[:, :width] = latent[...]
    packed[:, width:] = jnp.concatenate([key, key], axis=1)
    share = half.shape[0]
    half[...] = packed[pl.ds(pl.multiple_of(lax.rem(index[0], 2) * share, 16), share), :]
    blank = jnp.zeros((cos.shape[0], rot), BF16)
    wide = query_wide[...]
    narrow = query_narrow[...]
    size = NOPE_W + rot
    for h in range(2):
        head = wide[:, h * size : (h + 1) * size]
        queries[:, 256 * h : 256 * h + NOPE_W] = head[:, :NOPE_W]
        queries[:, 256 * h + NOPE_W : 256 * h + 256] = jnp.concatenate(
            [spun(head[:, NOPE_W:]), blank], axis=1
        )
    size = NOPE_N + rot
    first, second = narrow[:, :size], narrow[:, size:]
    queries[:, 512:640] = jnp.concatenate([first[:, :NOPE_N], spun(first[:, NOPE_N:])], axis=1)
    queries[:, 640:768] = jnp.concatenate([spun(second[:, NOPE_N:]), second[:, :NOPE_N]], axis=1)


def prepare(index, latent, rope_key, query_wide, query_narrow, cosine, sine):
    rows = latent.shape[0]
    return pl.pallas_call(
        prepare_kernel,
        out_shape=(
            jax.ShapeDtypeStruct((rows, latent.shape[1] + 128), BF16),
            jax.ShapeDtypeStruct((rows // 2, latent.shape[1] + 128), BF16),
            jax.ShapeDtypeStruct((rows, 768), BF16),
        ),
        in_specs=[SMEM] + [VMEM] * 6,
        out_specs=(VMEM,) * 3,
        name="prepare",
    )(index, latent, rope_key, query_wide, query_narrow, cosine, sine)


def attend_kernel(count, first, last, scales, *refs):
    q_own, q_other, key_wide, value_wide, key_narrow, value_narrow = refs[:6]
    pieces = refs[6 : 6 + count]
    old = None if first else refs[6 + count]
    outs = refs[-4 if last else -3 : -2]
    keys, values = refs[-2:]
    rows = q_own.shape[0]
    width = key_wide.shape[0]
    latent = jnp.concatenate([p[:, :width] for p in pieces], axis=0)
    turned = jnp.concatenate([p[:, width:] for p in pieces], axis=0)
    wide_keys = dot_nn(latent, key_wide[...]).astype(BF16)
    narrow_keys = dot_nn(latent, key_narrow[...]).astype(BF16)
    lane = lax.broadcasted_iota(jnp.int32, narrow_keys.shape, 1)
    keys[:, 0:128] = wide_keys[:, :128]
    keys[:, 128:256] = turned
    keys[:, 256:384] = wide_keys[:, 128:]
    keys[:, 384:512] = turned
    keys[:, 512:640] = jnp.where(lane < NOPE_N, narrow_keys, turned)
    keys[:, 640:768] = jnp.where(lane < NOPE_N, turned, narrow_keys)
    values[:, :256] = dot_nn(latent, value_wide[...]).astype(BF16)
    values[:, 256:] = dot_nn(latent, value_narrow[...]).astype(BF16)
    spans = [(0, 256), (256, 512), (512, 640), (640, 768)]
    out_lane = lax.broadcasted_iota(jnp.int32, (2 * rows, 128), 1)

    def put(begin, end, value):
        if last:
            outs[0][:, begin:end] = value[:rows]
            outs[1][:, begin:end] = value[rows:]
        else:
            outs[0][:, begin:end] = value

    stats = jnp.zeros((2 * rows, 128), F32)
    narrow_parts = []
    for h in range(4):
        begin, end = spans[h]
        place = min(h, 2) * 128
        factor = scales[h] * LOG2E
        q = jnp.concatenate([q_own[:, begin:end], q_other[:, begin:end]], axis=0)
        scores = dot_nt(q, keys[:, begin:end])
        top = jnp.max(scores, axis=1, keepdims=True)
        if not first:
            old_top = old[:, 384 + h : 385 + h]
            old_sum = old[:, 388 + h : 389 + h]
            top = jnp.maximum(top, old_top)
            shrink = jnp.exp2((old_top - top) * factor)
        prob = jnp.exp2((scores - top) * factor)
        total = jnp.sum(prob, axis=1, keepdims=True)
        mixed = dot_nn(prob.astype(BF16), values[:, place : place + 128])
        if not first:
            total = total + old_sum * shrink
            mixed = mixed + old[:, place : place + 128] * shrink
        stats = jnp.where(out_lane == h, top, stats)
        stats = jnp.where(out_lane == 4 + h, total, stats)
        if h < 2:
            put(place, place + 128, mixed)
        else:
            narrow_parts.append(mixed)
    put(256, 384, jnp.where(out_lane < NOPE_N, narrow_parts[0], narrow_parts[1]))
    put(384, 512, stats)


def attend(queries, weights, pieces, state, scales, last=False):
    rows = queries[0].shape[0]
    keys = sum(p.shape[0] for p in pieces)
    first = state is None
    operands = [*queries, *weights, *pieces, *(() if first else (state,))]
    side = jax.ShapeDtypeStruct((rows, 512), F32)
    both = jax.ShapeDtypeStruct((2 * rows, 512), F32)
    return pl.pallas_call(
        functools.partial(attend_kernel, len(pieces), first, last, scales),
        out_shape=(side, side) if last else both,
        in_specs=[VMEM] * len(operands),
        out_specs=(VMEM, VMEM) if last else VMEM,
        scratch_shapes=[pltpu.VMEM((keys, 768), BF16), pltpu.VMEM((keys, 384), BF16)],
        cost_estimate=pl.CostEstimate(
            flops=2 * keys * (512 * 768 + 2 * rows * 1280),
            bytes_accessed=8 * rows * 512 + 2 * keys * 640 + 2 * 512 * 768,
            transcendentals=8 * rows * keys,
        ),
        name="attend",
    )(*operands)


def project_kernel(parts, scales, index, mine, theirs, out_wide, out_narrow, *refs):
    outs, scratch = refs[:parts], refs[parts]
    rows = mine.shape[0]
    lane = lax.broadcasted_iota(jnp.int32, (rows, 128), 1)
    pieces = []
    for h in range(4):
        factor = scales[h] * LOG2E
        top_a, top_b = mine[:, 384 + h : 385 + h], theirs[:, 384 + h : 385 + h]
        sum_a, sum_b = mine[:, 388 + h : 389 + h], theirs[:, 388 + h : 389 + h]
        top = jnp.maximum(top_a, top_b)
        shrink_a = jnp.exp2((top_a - top) * factor)
        shrink_b = jnp.exp2((top_b - top) * factor)
        total = sum_a * shrink_a + sum_b * shrink_b
        place = min(h, 2) * 128
        mixed = mine[:, place : place + 128] * shrink_a + theirs[:, place : place + 128] * shrink_b
        pieces.append(mixed / total)
    narrow = jnp.where(lane < NOPE_N, pieces[2], pieces[3])
    wide = jnp.concatenate(pieces[:2], axis=1).astype(BF16)
    scratch[...] = dot_nn(wide, out_wide[...]) + dot_nn(narrow.astype(BF16), out_narrow[...])
    share = rows // parts
    for d in range(parts):
        block = lax.rem(index[0] + d, parts)
        start = pl.multiple_of(block * share, 16)
        outs[d][...] = scratch[pl.ds(start, share), :].astype(BF16)


def project(index, mine, theirs, out_wide, out_narrow, parts, scales):
    rows, width = mine.shape[0], out_wide.shape[1]
    shape = jax.ShapeDtypeStruct((rows // parts, width), BF16)
    return pl.pallas_call(
        functools.partial(project_kernel, parts, scales),
        out_shape=(shape,) * parts,
        in_specs=[SMEM] + [VMEM] * 4,
        out_specs=(VMEM,) * parts,
        scratch_shapes=[pltpu.VMEM((rows, width), F32)],
        cost_estimate=pl.CostEstimate(
            flops=2 * rows * width * 384, bytes_accessed=4 * rows * width, transcendentals=0
        ),
        name="project",
    )(index, mine, theirs, out_wide, out_narrow)


def mixer_kernel(parts, cuts, out_step, index, taps, before, after, *refs):
    blocks, weights = refs[:parts], refs[parts]
    outs = refs[parts + 1 : 2 * parts + 1]
    x, w_gate, w_value, w_down, gate, hidden, terms, sems = refs[2 * parts + 1 :]
    width, units = w_gate.shape
    at_tp = index[0]
    chunks = list(zip(cuts, cuts[1:]))
    copies = []
    for n, (begin, end) in enumerate(chunks):
        for which, target in enumerate((w_gate, w_value)):
            source = weights.at[:, which * units + begin : which * units + end]
            copies.append(
                pltpu.make_async_copy(source, target.at[:, begin:end], sems.at[which, n])
            )
    out_cuts = list(range(0, width, out_step))
    for n, begin in enumerate(out_cuts):
        source = weights.at[begin : begin + out_step, 2 * units :]
        copies.append(
            pltpu.make_async_copy(source, w_down.at[begin : begin + out_step, :], sems.at[2, n])
        )
    for copy in copies:
        copy.start()
    share = blocks[0].shape[0]
    rows = parts * share
    x[:HALO, :] = before[...]
    x[HALO + rows :, :] = after[...]
    for d in range(parts):
        block = lax.rem(at_tp - d + parts, parts)
        start = pl.multiple_of(HALO + block * share, 16)
        x[pl.ds(start, share), :] = blocks[d][...]
    for n, (begin, end) in enumerate(chunks):
        copies[2 * n].wait()
        gate[:, : end - begin] = dot_nn(x[...], w_gate[:, begin:end]).astype(BF16).astype(F32)
        copies[2 * n + 1].wait()
        value = dot_nn(x[HALO : HALO + rows, :], w_value[:, begin:end])
        mixed = jnp.zeros_like(value)
        for tap in range(taps.shape[0]):
            first = HALO - 1 + tap
            mixed = mixed + taps[tap : tap + 1, begin:end] * gate[first : first + rows, : end - begin]
        hidden[:, begin:end] = (mixed / (1.0 + jnp.exp(-mixed)) * value).astype(BF16)
    for n, begin in enumerate(out_cuts):
        copies[2 * len(chunks) + n].wait()
        terms[:, begin : begin + out_step] = dot_nt(hidden[...], w_down[begin : begin + out_step, :])
    for d in range(parts):
        block = lax.rem(at_tp + d, parts)
        start = pl.multiple_of(block * share, 16)
        outs[d][...] = terms[pl.ds(start, share), :].astype(BF16)


def mixer(index, taps, before, after, blocks, weights):
    parts = len(blocks)
    share, width = blocks[0].shape
    rows = parts * share
    units = weights.shape[1] // 3
    cuts = tuple(range(0, units, 384)) + (units,)
    out_step = width // 4
    return pl.pallas_call(
        functools.partial(mixer_kernel, parts, cuts, out_step),
        out_shape=(jax.ShapeDtypeStruct((share, width), BF16),) * parts,
        in_specs=[SMEM] + [VMEM] * (3 + parts) + [ANY],
        out_specs=(VMEM,) * parts,
        scratch_shapes=[
            pltpu.VMEM((2 * HALO + rows, width), BF16),
            pltpu.VMEM((width, units), BF16),
            pltpu.VMEM((width, units), BF16),
            pltpu.VMEM((width, units), BF16),
            pltpu.VMEM((2 * HALO + rows, 384), F32),
            pltpu.VMEM((rows, units), BF16),
            pltpu.VMEM((rows, width), F32),
            pltpu.SemaphoreType.DMA((3, max(len(cuts) - 1, 4))),
        ],
        cost_estimate=pl.CostEstimate(
            flops=6 * rows * width * units,
            bytes_accessed=6 * width * units,
            transcendentals=rows * units,
        ),
        name="mixer",
    )(index, taps, before, after, *blocks, weights)


def fence(live):
    names = list(live)
    return dict(zip(names, lax.optimization_barrier(tuple(live[n] for n in names))))


def on_device(
    layer_input,
    latent,
    rope_key,
    query_wide,
    query_narrow,
    key_up_wide,
    value_up_wide,
    key_up_narrow,
    value_up_narrow,
    out_wide,
    out_narrow,
    norm_gain,
    gate_weight,
    value_weight,
    conv_weight,
    down_weight,
):
    n_sp, n_tp = lax.axis_size("sp"), lax.axis_size("tp")
    n_z = n_sp // CORES
    steps = {"up": n_z // 2, "down": n_z - 1 - n_z // 2}
    at_sp, at_tp = lax.axis_index("sp"), lax.axis_index("tp")
    index = at_tp.astype(jnp.int32)[None]
    z_moves = {"up": shift_perm(n_sp, CORES), "down": shift_perm(n_sp, -CORES)}
    x_moves = {"up": shift_perm(n_tp, 1), "down": shift_perm(n_tp, -1)}
    swap = partner_perm(n_sp)
    rows = latent.shape[0]
    rot = rope_key.shape[1]
    wide_scale = 1.0 / math.sqrt(NOPE_W + rot)
    narrow_scale = 1.0 / math.sqrt(NOPE_N + rot)
    scales = (wide_scale, wide_scale, narrow_scale, narrow_scale)
    up_weights = (key_up_wide, value_up_wide, key_up_narrow, value_up_narrow)

    stacked = jnp.concatenate([gate_weight, value_weight, down_weight.T], axis=1)
    weights = None

    cosine, sine = rope_tables(at_sp * rows, rows, rot)
    packed, half, q_own = prepare(
        index, latent, rope_key, query_wide, query_narrow, cosine, sine
    )
    live = {"up": half, "down": half, "q": q_own, "stacked": stacked}
    arrived, held = [packed], {"up": [], "down": []}
    state = None
    last = steps["up"]
    batch_ticks = (last // 2 + 1, last, last + 1)
    for tick in range(1, last + 2):
        new = {}
        if tick in batch_ticks:
            for way in ("up", "down"):
                pieces = [live[n] for n in held[way]]
                if not pieces:
                    continue
                joined = pieces[0] if len(pieces) == 1 else jnp.concatenate(pieces, axis=0)
                new["x" + way] = lax.ppermute(joined, "tp", x_moves[way])
        for way in ("up", "down"):
            if tick <= steps[way]:
                new[way] = lax.ppermute(live[way], "sp", z_moves[way])
        if tick == 1:
            new["q_other"] = lax.ppermute(live["q"], "sp", swap)
        if tick in batch_ticks:
            queries = (live["q"], live["q_other"])
            new["state"] = attend(queries, up_weights, arrived, state, scales)
            arrived, held = [], {"up": [], "down": []}
        for name in live:
            kept = name in ("q", "q_other", "stacked") or name in held["up"] + held["down"]
            if name not in new and kept:
                new[name] = live[name]
        live = fence(new)
        if tick == GATHER_AFTER:
            weights = lax.all_gather(live.pop("stacked"), "sp", axis=0, tiled=True)
        state = live.get("state", state)
        for way in ("up", "down"):
            if tick <= steps[way]:
                arrived.append(live[way])
                held[way].append(f"{way}{tick}")
                live[f"{way}{tick}"] = live[way]
            if "x" + way in live:
                arrived.append(live["x" + way])
    queries = (live["q"], live["q_other"])
    state = attend(queries, up_weights, arrived, state, scales, last=True)
    theirs = lax.ppermute(state[1], "sp", swap)
    blocks = project(index, state[0], theirs, out_wide, out_narrow, n_tp, scales)

    total = blocks[0].astype(F32)
    for d in range(1, n_tp):
        total = total + lax.ppermute(blocks[d], "tp", shift_perm(n_tp, d)).astype(F32)
    middle = (layer_input.astype(F32) + total).astype(BF16)
    full = middle.astype(F32)
    scale = lax.rsqrt(jnp.mean(full * full, axis=-1, keepdims=True) + norm_eps)
    normed = (full * scale * norm_gain).astype(BF16)
    blocks = [normed] + [
        lax.ppermute(normed, "tp", shift_perm(n_tp, d)) for d in range(1, n_tp)
    ]
    tails = jnp.stack([b[-HALO:] for b in blocks])
    heads = jnp.stack([b[:HALO] for b in blocks])
    tail = lax.dynamic_index_in_dim(tails, (at_tp + 1) % n_tp, 0, False)
    head = lax.dynamic_index_in_dim(heads, at_tp, 0, False)
    odd = at_sp % CORES == 1
    outward = [(i, i + 1) for i in range(1, n_sp - 1, CORES)]
    outward = outward + [(j, i) for i, j in outward]
    across = lax.ppermute(jnp.where(odd, tail, head), "sp", outward)
    within = lax.ppermute(jnp.where(odd, head, tail), "sp", swap)
    before = jnp.where(odd, within, across)
    after = jnp.where(odd, across, within)
    blocks, before, after, weights = lax.optimization_barrier((blocks, before, after, weights))
    terms = mixer(index, conv_weight, before, after, blocks, weights)
    total = terms[0].astype(F32)
    for d in range(1, n_tp):
        total = total + lax.ppermute(terms[d], "tp", shift_perm(n_tp, d)).astype(F32)
    return (middle.astype(F32) + total).astype(BF16)


def solution(mesh):
    in_specs = (
        P(("grp", "sp", "tp"), None),
        P(("grp", "sp"), None),
        P(("grp", "sp"), None),
        P(("grp", "sp"), "tp"),
        P(("grp", "sp"), "tp"),
        P(None, "tp"),
        P(None, "tp"),
        P(None, "tp"),
        P(None, "tp"),
        P("tp", None),
        P("tp", None),
        P(),
        P("sp", "tp"),
        P("sp", "tp"),
        P(None, "tp"),
        P("tp", "sp"),
    )
    out_specs = P(("grp", "sp", "tp"), None)
    return jax.shard_map(
        on_device, mesh=mesh, in_specs=in_specs, out_specs=out_specs, check_vma=False
    )
```

```python
import functools
import math

import jax
import jax.numpy as jnp
from jax import lax
from jax.experimental import pallas as pl
from jax.experimental.pallas import tpu as pltpu
from jax.sharding import PartitionSpec as P

NOPE_W = 128
NOPE_N = 64
CORES = 2
HALO = 16
GATHER_AFTER = 3
LOG2E = math.log2(math.e)

rope_base = 10000.0
norm_eps = 1e-06


F32 = jnp.float32
BF16 = jnp.bfloat16
VMEM = pl.BlockSpec(memory_space=pltpu.VMEM)
SMEM = pl.BlockSpec(memory_space=pltpu.SMEM)
ANY = pl.BlockSpec(memory_space=pl.ANY)


def shift_perm(size, by):
    return [(i, (i + by) % size) for i in range(size)]


def partner_perm(size):
    return [(i, i ^ 1) for i in range(size)]


def fetch(sources, targets, sems):
    copies = [
        pltpu.make_async_copy(source, target, sems.at[i])
        for i, (source, target) in enumerate(zip(sources, targets))
    ]
    for copy in copies:
        copy.start()
    for copy in copies:
        copy.wait()


def dot_nt(a, b):
    return lax.dot_general(a, b, (((1,), (1,)), ((), ())), preferred_element_type=F32)


def dot_nn(a, b):
    return jnp.dot(a, b, preferred_element_type=F32)


def rope_tables(row_start, row_total, span_width):
    places = (row_start + jnp.arange(row_total, dtype=jnp.int32)).astype(F32)
    frequency = jnp.power(
        rope_base, -jnp.arange(0, span_width, 2, dtype=jnp.int32).astype(F32) / span_width
    )
    angles = places[:, None] * frequency[None, :]
    angles = jnp.concatenate([angles, angles], axis=-1)
    return (jnp.cos(angles), jnp.sin(angles))


def prepare_kernel(
    index, latent, rope_key, query_wide, query_narrow, cosine, sine, packed, half, queries
):
    cos, sin = cosine[...], sine[...]
    rot = cos.shape[1]

    def spun(entries):
        entries = entries.astype(F32)
        half = rot // 2
        turned = jnp.concatenate([-entries[:, half:], entries[:, :half]], axis=1)
        return (entries * cos + turned * sin).astype(BF16)

    key = spun(rope_key[...])
    width = latent.shape[1]
    packed[:, :width] = latent[...]
    packed[:, width:] = jnp.concatenate([key, key], axis=1)
    share = half.shape[0]
    half[...] = packed[pl.ds(pl.multiple_of(lax.rem(index[0], 2) * share, 16), share), :]
    blank = jnp.zeros((cos.shape[0], rot), BF16)
    wide = query_wide[...]
    narrow = query_narrow[...]
    size = NOPE_W + rot
    for h in range(2):
        head = wide[:, h * size : (h + 1) * size]
        queries[:, 256 * h : 256 * h + NOPE_W] = head[:, :NOPE_W]
        queries[:, 256 * h + NOPE_W : 256 * h + 256] = jnp.concatenate(
            [spun(head[:, NOPE_W:]), blank], axis=1
        )
    size = NOPE_N + rot
    first, second = narrow[:, :size], narrow[:, size:]
    queries[:, 512:640] = jnp.concatenate([first[:, :NOPE_N], spun(first[:, NOPE_N:])], axis=1)
    queries[:, 640:768] = jnp.concatenate([spun(second[:, NOPE_N:]), second[:, :NOPE_N]], axis=1)


def prepare(index, latent, rope_key, query_wide, query_narrow, cosine, sine):
    rows = latent.shape[0]
    return pl.pallas_call(
        prepare_kernel,
        out_shape=(
            jax.ShapeDtypeStruct((rows, latent.shape[1] + 128), BF16),
            jax.ShapeDtypeStruct((rows // 2, latent.shape[1] + 128), BF16),
            jax.ShapeDtypeStruct((rows, 768), BF16),
        ),
        in_specs=[SMEM] + [VMEM] * 6,
        out_specs=(VMEM,) * 3,
        name="prepare",
    )(index, latent, rope_key, query_wide, query_narrow, cosine, sine)


def attend_kernel(count, first, last, scales, *refs):
    fetched = 6 + count + (0 if first else 1)
    outs = refs[fetched : fetched + (2 if last else 1)]
    q, key_wide, value_wide, key_narrow, value_narrow, joined, old, keys, values, sems = refs[-10:]
    rows = q.shape[0] // 2
    width = key_wide.shape[0]
    targets = [q.at[:rows], q.at[rows:], key_wide, value_wide, key_narrow, value_narrow]
    begin = 0
    for piece in refs[6 : 6 + count]:
        targets.append(joined.at[begin : begin + piece.shape[0], :])
        begin += piece.shape[0]
    if not first:
        targets.append(old)
    fetch(refs[:fetched], targets, sems)
    latent = joined[:, :width]
    turned = joined[:, width:]
    wide_keys = dot_nn(latent, key_wide[...]).astype(BF16)
    narrow_keys = dot_nn(latent, key_narrow[...]).astype(BF16)
    lane = lax.broadcasted_iota(jnp.int32, narrow_keys.shape, 1)
    keys[:, 0:128] = wide_keys[:, :128]
    keys[:, 128:256] = turned
    keys[:, 256:384] = wide_keys[:, 128:]
    keys[:, 384:512] = turned
    keys[:, 512:640] = jnp.where(lane < NOPE_N, narrow_keys, turned)
    keys[:, 640:768] = jnp.where(lane < NOPE_N, turned, narrow_keys)
    values[:, :256] = dot_nn(latent, value_wide[...]).astype(BF16)
    values[:, 256:] = dot_nn(latent, value_narrow[...]).astype(BF16)
    spans = [(0, 256), (256, 512), (512, 640), (640, 768)]
    out_lane = lax.broadcasted_iota(jnp.int32, (2 * rows, 128), 1)

    def put(begin, end, value):
        if last:
            outs[0][:, begin:end] = value[:rows]
            outs[1][:, begin:end] = value[rows:]
        else:
            outs[0][:, begin:end] = value

    stats = jnp.zeros((2 * rows, 128), F32)
    narrow_parts = []
    for h in range(4):
        begin, end = spans[h]
        place = min(h, 2) * 128
        factor = scales[h] * LOG2E
        scores = dot_nt(q[:, begin:end], keys[:, begin:end])
        top = jnp.max(scores, axis=1, keepdims=True)
        if not first:
            old_top = old[:, 384 + h : 385 + h]
            old_sum = old[:, 388 + h : 389 + h]
            top = jnp.maximum(top, old_top)
            shrink = jnp.exp2((old_top - top) * factor)
        prob = jnp.exp2((scores - top) * factor)
        total = jnp.sum(prob, axis=1, keepdims=True)
        mixed = dot_nn(prob.astype(BF16), values[:, place : place + 128])
        if not first:
            total = total + old_sum * shrink
            mixed = mixed + old[:, place : place + 128] * shrink
        stats = jnp.where(out_lane == h, top, stats)
        stats = jnp.where(out_lane == 4 + h, total, stats)
        if h < 2:
            put(place, place + 128, mixed)
        else:
            narrow_parts.append(mixed)
    put(256, 384, jnp.where(out_lane < NOPE_N, narrow_parts[0], narrow_parts[1]))
    put(384, 512, stats)


def attend(queries, weights, pieces, state, scales, last=False):
    rows = queries[0].shape[0]
    keys = sum(p.shape[0] for p in pieces)
    first = state is None
    operands = [*queries, *weights, *pieces, *(() if first else (state,))]
    side = jax.ShapeDtypeStruct((rows, 512), F32)
    both = jax.ShapeDtypeStruct((2 * rows, 512), F32)
    return pl.pallas_call(
        functools.partial(attend_kernel, len(pieces), first, last, scales),
        out_shape=(side, side) if last else both,
        in_specs=[ANY] * len(operands),
        out_specs=(VMEM, VMEM) if last else VMEM,
        scratch_shapes=[
            pltpu.VMEM((2 * rows, 768), BF16),
            *(pltpu.VMEM(w.shape, BF16) for w in weights),
            pltpu.VMEM((keys, pieces[0].shape[1]), BF16),
            pltpu.VMEM((2 * rows, 512), F32),
            pltpu.VMEM((keys, 768), BF16),
            pltpu.VMEM((keys, 384), BF16),
            pltpu.SemaphoreType.DMA((len(operands),)),
        ],
        cost_estimate=pl.CostEstimate(
            flops=2 * keys * (512 * 768 + 2 * rows * 1280),
            bytes_accessed=8 * rows * 512 + 2 * keys * 640 + 2 * 512 * 768,
            transcendentals=8 * rows * keys,
        ),
        name="attend",
    )(*operands)


def project_kernel(parts, scales, index, *refs):
    outs = refs[4 : 4 + parts]
    mine, theirs, out_wide, out_narrow, scratch, sems = refs[4 + parts :]
    fetch(refs[:4], (mine, theirs, out_wide, out_narrow), sems)
    rows = mine.shape[0]
    lane = lax.broadcasted_iota(jnp.int32, (rows, 128), 1)
    pieces = []
    for h in range(4):
        factor = scales[h] * LOG2E
        top_a, top_b = mine[:, 384 + h : 385 + h], theirs[:, 384 + h : 385 + h]
        sum_a, sum_b = mine[:, 388 + h : 389 + h], theirs[:, 388 + h : 389 + h]
        top = jnp.maximum(top_a, top_b)
        shrink_a = jnp.exp2((top_a - top) * factor)
        shrink_b = jnp.exp2((top_b - top) * factor)
        total = sum_a * shrink_a + sum_b * shrink_b
        place = min(h, 2) * 128
        mixed = mine[:, place : place + 128] * shrink_a + theirs[:, place : place + 128] * shrink_b
        pieces.append(mixed / total)
    narrow = jnp.where(lane < NOPE_N, pieces[2], pieces[3])
    wide = jnp.concatenate(pieces[:2], axis=1).astype(BF16)
    scratch[...] = dot_nn(wide, out_wide[...]) + dot_nn(narrow.astype(BF16), out_narrow[...])
    share = rows // parts
    for d in range(parts):
        block = lax.rem(index[0] + d, parts)
        start = pl.multiple_of(block * share, 16)
        outs[d][...] = scratch[pl.ds(start, share), :].astype(BF16)


def project(index, mine, theirs, out_wide, out_narrow, parts, scales):
    rows, width = mine.shape[0], out_wide.shape[1]
    shape = jax.ShapeDtypeStruct((rows // parts, width), BF16)
    return pl.pallas_call(
        functools.partial(project_kernel, parts, scales),
        out_shape=(shape,) * parts,
        in_specs=[SMEM] + [ANY] * 4,
        out_specs=(VMEM,) * parts,
        scratch_shapes=[
            pltpu.VMEM(mine.shape, F32),
            pltpu.VMEM(theirs.shape, F32),
            pltpu.VMEM(out_wide.shape, BF16),
            pltpu.VMEM(out_narrow.shape, BF16),
            pltpu.VMEM((rows, width), F32),
            pltpu.SemaphoreType.DMA((4,)),
        ],
        cost_estimate=pl.CostEstimate(
            flops=2 * rows * width * 384, bytes_accessed=4 * rows * width, transcendentals=0
        ),
        name="project",
    )(index, mine, theirs, out_wide, out_narrow)


def mixer_kernel(parts, cuts, out_step, index, taps, before, after, *refs):
    blocks, weights = refs[:parts], refs[parts]
    outs = refs[parts + 1 : 2 * parts + 1]
    x, w_gate, w_value, w_down, gate, hidden, terms, sems = refs[2 * parts + 1 :]
    width, units = w_gate.shape
    at_tp = index[0]
    chunks = list(zip(cuts, cuts[1:]))
    copies = []
    for n, (begin, end) in enumerate(chunks):
        for which, target in enumerate((w_gate, w_value)):
            source = weights.at[:, which * units + begin : which * units + end]
            copies.append(
                pltpu.make_async_copy(source, target.at[:, begin:end], sems.at[which, n])
            )
    out_cuts = list(range(0, width, out_step))
    for n, begin in enumerate(out_cuts):
        source = weights.at[begin : begin + out_step, 2 * units :]
        copies.append(
            pltpu.make_async_copy(source, w_down.at[begin : begin + out_step, :], sems.at[2, n])
        )
    share = blocks[0].shape[0]
    rows = parts * share
    inputs = [
        pltpu.make_async_copy(before, x.at[:HALO, :], sems.at[3, 0]),
        pltpu.make_async_copy(after, x.at[HALO + rows :, :], sems.at[3, 1]),
    ]
    for d in range(parts):
        block = lax.rem(at_tp - d + parts, parts)
        start = pl.multiple_of(HALO + block * share, 16)
        inputs.append(
            pltpu.make_async_copy(blocks[d], x.at[pl.ds(start, share), :], sems.at[3, 2 + d])
        )
    for copy in inputs + copies:
        copy.start()
    for copy in inputs:
        copy.wait()
    for n, (begin, end) in enumerate(chunks):
        copies[2 * n].wait()
        gate[:, : end - begin] = dot_nn(x[...], w_gate[:, begin:end]).astype(BF16).astype(F32)
        copies[2 * n + 1].wait()
        value = dot_nn(x[HALO : HALO + rows, :], w_value[:, begin:end])
        mixed = jnp.zeros_like(value)
        for tap in range(taps.shape[0]):
            first = HALO - 1 + tap
            mixed = mixed + taps[tap : tap + 1, begin:end] * gate[first : first + rows, : end - begin]
        hidden[:, begin:end] = (mixed / (1.0 + jnp.exp(-mixed)) * value).astype(BF16)
    for n, begin in enumerate(out_cuts):
        copies[2 * len(chunks) + n].wait()
        terms[:, begin : begin + out_step] = dot_nt(hidden[...], w_down[begin : begin + out_step, :])
    for d in range(parts):
        block = lax.rem(at_tp + d, parts)
        start = pl.multiple_of(block * share, 16)
        outs[d][...] = terms[pl.ds(start, share), :].astype(BF16)


def mixer(index, taps, before, after, blocks, weights):
    parts = len(blocks)
    share, width = blocks[0].shape
    rows = parts * share
    units = weights.shape[1] // 3
    cuts = tuple(range(0, units, 384)) + (units,)
    out_step = width // 4
    return pl.pallas_call(
        functools.partial(mixer_kernel, parts, cuts, out_step),
        out_shape=(jax.ShapeDtypeStruct((share, width), BF16),) * parts,
        in_specs=[SMEM, VMEM] + [ANY] * (3 + parts),
        out_specs=(VMEM,) * parts,
        scratch_shapes=[
            pltpu.VMEM((2 * HALO + rows, width), BF16),
            pltpu.VMEM((width, units), BF16),
            pltpu.VMEM((width, units), BF16),
            pltpu.VMEM((width, units), BF16),
            pltpu.VMEM((2 * HALO + rows, 384), F32),
            pltpu.VMEM((rows, units), BF16),
            pltpu.VMEM((rows, width), F32),
            pltpu.SemaphoreType.DMA((4, max(len(cuts) - 1, 4, 2 + parts))),
        ],
        cost_estimate=pl.CostEstimate(
            flops=6 * rows * width * units,
            bytes_accessed=6 * width * units,
            transcendentals=rows * units,
        ),
        name="mixer",
    )(index, taps, before, after, *blocks, weights)


def fence(live):
    names = list(live)
    return dict(zip(names, lax.optimization_barrier(tuple(live[n] for n in names))))


def on_device(
    layer_input,
    latent,
    rope_key,
    query_wide,
    query_narrow,
    key_up_wide,
    value_up_wide,
    key_up_narrow,
    value_up_narrow,
    out_wide,
    out_narrow,
    norm_gain,
    gate_weight,
    value_weight,
    conv_weight,
    down_weight,
):
    n_sp, n_tp = lax.axis_size("sp"), lax.axis_size("tp")
    n_z = n_sp // CORES
    steps = {"up": n_z // 2, "down": n_z - 1 - n_z // 2}
    at_sp, at_tp = lax.axis_index("sp"), lax.axis_index("tp")
    index = at_tp.astype(jnp.int32)[None]
    z_moves = {"up": shift_perm(n_sp, CORES), "down": shift_perm(n_sp, -CORES)}
    x_moves = {"up": shift_perm(n_tp, 1), "down": shift_perm(n_tp, -1)}
    swap = partner_perm(n_sp)
    rows = latent.shape[0]
    rot = rope_key.shape[1]
    wide_scale = 1.0 / math.sqrt(NOPE_W + rot)
    narrow_scale = 1.0 / math.sqrt(NOPE_N + rot)
    scales = (wide_scale, wide_scale, narrow_scale, narrow_scale)
    up_weights = (key_up_wide, value_up_wide, key_up_narrow, value_up_narrow)

    stacked = jnp.concatenate([gate_weight, value_weight, down_weight.T], axis=1)
    weights = None

    cosine, sine = rope_tables(at_sp * rows, rows, rot)
    packed, half, q_own = prepare(
        index, latent, rope_key, query_wide, query_narrow, cosine, sine
    )
    live = {"up": half, "down": half, "q": q_own, "stacked": stacked}
    arrived, held = [packed], {"up": [], "down": []}
    state = None
    last = steps["up"]
    batch_ticks = (last // 2 + 1, last, last + 1)
    for tick in range(1, last + 2):
        new = {}
        if tick in batch_ticks:
            for way in ("up", "down"):
                pieces = [live[n] for n in held[way]]
                if not pieces:
                    continue
                joined = pieces[0] if len(pieces) == 1 else jnp.concatenate(pieces, axis=0)
                new["x" + way] = lax.ppermute(joined, "tp", x_moves[way])
        for way in ("up", "down"):
            if tick <= steps[way]:
                new[way] = lax.ppermute(live[way], "sp", z_moves[way])
        if tick == 1:
            new["q_other"] = lax.ppermute(live["q"], "sp", swap)
        if tick in batch_ticks:
            queries = (live["q"], live["q_other"])
            new["state"] = attend(queries, up_weights, arrived, state, scales)
            arrived, held = [], {"up": [], "down": []}
        for name in live:
            kept = name in ("q", "q_other", "stacked") or name in held["up"] + held["down"]
            if name not in new and kept:
                new[name] = live[name]
        live = fence(new)
        if tick == GATHER_AFTER:
            weights = lax.all_gather(live.pop("stacked"), "sp", axis=0, tiled=True)
        state = live.get("state", state)
        for way in ("up", "down"):
            if tick <= steps[way]:
                arrived.append(live[way])
                held[way].append(f"{way}{tick}")
                live[f"{way}{tick}"] = live[way]
            if "x" + way in live:
                arrived.append(live["x" + way])
    queries = (live["q"], live["q_other"])
    state = attend(queries, up_weights, arrived, state, scales, last=True)
    theirs = lax.ppermute(state[1], "sp", swap)
    blocks = project(index, state[0], theirs, out_wide, out_narrow, n_tp, scales)

    total = blocks[0].astype(F32)
    for d in range(1, n_tp):
        total = total + lax.ppermute(blocks[d], "tp", shift_perm(n_tp, d)).astype(F32)
    middle = (layer_input.astype(F32) + total).astype(BF16)
    full = middle.astype(F32)
    scale = lax.rsqrt(jnp.mean(full * full, axis=-1, keepdims=True) + norm_eps)
    normed = (full * scale * norm_gain).astype(BF16)
    blocks = [normed] + [
        lax.ppermute(normed, "tp", shift_perm(n_tp, d)) for d in range(1, n_tp)
    ]
    tails = jnp.stack([b[-HALO:] for b in blocks])
    heads = jnp.stack([b[:HALO] for b in blocks])
    tail = lax.dynamic_index_in_dim(tails, (at_tp + 1) % n_tp, 0, False)
    head = lax.dynamic_index_in_dim(heads, at_tp, 0, False)
    odd = at_sp % CORES == 1
    outward = [(i, i + 1) for i in range(1, n_sp - 1, CORES)]
    outward = outward + [(j, i) for i, j in outward]
    across = lax.ppermute(jnp.where(odd, tail, head), "sp", outward)
    within = lax.ppermute(jnp.where(odd, head, tail), "sp", swap)
    before = jnp.where(odd, within, across)
    after = jnp.where(odd, across, within)
    blocks, before, after, weights = lax.optimization_barrier((blocks, before, after, weights))
    terms = mixer(index, conv_weight, before, after, blocks, weights)
    total = terms[0].astype(F32)
    for d in range(1, n_tp):
        total = total + lax.ppermute(terms[d], "tp", shift_perm(n_tp, d)).astype(F32)
    return (middle.astype(F32) + total).astype(BF16)


def solution(mesh):
    in_specs = (
        P(("grp", "sp", "tp"), None),
        P(("grp", "sp"), None),
        P(("grp", "sp"), None),
        P(("grp", "sp"), "tp"),
        P(("grp", "sp"), "tp"),
        P(None, "tp"),
        P(None, "tp"),
        P(None, "tp"),
        P(None, "tp"),
        P("tp", None),
        P("tp", None),
        P(),
        P("sp", "tp"),
        P("sp", "tp"),
        P(None, "tp"),
        P("tp", "sp"),
    )
    out_specs = P(("grp", "sp", "tp"), None)
    return jax.shard_map(
        on_device, mesh=mesh, in_specs=in_specs, out_specs=out_specs, check_vma=False
    )
```

```python
import functools
import math

import jax
import jax.numpy as jnp
from jax import lax
from jax.experimental import pallas as pl
from jax.experimental.pallas import tpu as pltpu
from jax.sharding import PartitionSpec as P

NOPE_W = 128
NOPE_N = 64
CORES = 2
HALO = 16
GATHER_AFTER = 2
LOG2E = math.log2(math.e)

rope_base = 10000.0
norm_eps = 1e-06


F32 = jnp.float32
BF16 = jnp.bfloat16
VMEM = pl.BlockSpec(memory_space=pltpu.VMEM)
SMEM = pl.BlockSpec(memory_space=pltpu.SMEM)
ANY = pl.BlockSpec(memory_space=pl.ANY)


def shift_perm(size, by):
    return [(i, (i + by) % size) for i in range(size)]


def partner_perm(size):
    return [(i, i ^ 1) for i in range(size)]


def fetch(sources, targets, sems):
    copies = [
        pltpu.make_async_copy(source, target, sems.at[i])
        for i, (source, target) in enumerate(zip(sources, targets))
    ]
    for copy in copies:
        copy.start()
    for copy in copies:
        copy.wait()


def dot_nt(a, b):
    return lax.dot_general(a, b, (((1,), (1,)), ((), ())), preferred_element_type=F32)


def dot_nn(a, b):
    return jnp.dot(a, b, preferred_element_type=F32)


def rope_tables(row_start, row_total, span_width):
    places = (row_start + jnp.arange(row_total, dtype=jnp.int32)).astype(F32)
    frequency = jnp.power(
        rope_base, -jnp.arange(0, span_width, 2, dtype=jnp.int32).astype(F32) / span_width
    )
    angles = places[:, None] * frequency[None, :]
    angles = jnp.concatenate([angles, angles], axis=-1)
    return (jnp.cos(angles), jnp.sin(angles))


def prepare_kernel(
    index, latent, rope_key, query_wide, query_narrow, cosine, sine, packed, half, queries
):
    cos, sin = cosine[...], sine[...]
    rot = cos.shape[1]

    def spun(entries):
        entries = entries.astype(F32)
        half = rot // 2
        turned = jnp.concatenate([-entries[:, half:], entries[:, :half]], axis=1)
        return (entries * cos + turned * sin).astype(BF16)

    key = spun(rope_key[...])
    width = latent.shape[1]
    packed[:, :width] = latent[...]
    packed[:, width:] = jnp.concatenate([key, key], axis=1)
    share = half.shape[0]
    half[...] = packed[pl.ds(pl.multiple_of(lax.rem(index[0], 2) * share, 16), share), :]
    blank = jnp.zeros((cos.shape[0], rot), BF16)
    wide = query_wide[...]
    narrow = query_narrow[...]
    size = NOPE_W + rot
    for h in range(2):
        head = wide[:, h * size : (h + 1) * size]
        queries[:, 256 * h : 256 * h + NOPE_W] = head[:, :NOPE_W]
        queries[:, 256 * h + NOPE_W : 256 * h + 256] = jnp.concatenate(
            [spun(head[:, NOPE_W:]), blank], axis=1
        )
    size = NOPE_N + rot
    first, second = narrow[:, :size], narrow[:, size:]
    queries[:, 512:640] = jnp.concatenate([first[:, :NOPE_N], spun(first[:, NOPE_N:])], axis=1)
    queries[:, 640:768] = jnp.concatenate([spun(second[:, NOPE_N:]), second[:, :NOPE_N]], axis=1)


def prepare(index, latent, rope_key, query_wide, query_narrow, cosine, sine):
    rows = latent.shape[0]
    return pl.pallas_call(
        prepare_kernel,
        out_shape=(
            jax.ShapeDtypeStruct((rows, latent.shape[1] + 128), BF16),
            jax.ShapeDtypeStruct((rows // 2, latent.shape[1] + 128), BF16),
            jax.ShapeDtypeStruct((rows, 768), BF16),
        ),
        in_specs=[SMEM] + [VMEM] * 6,
        out_specs=(VMEM,) * 3,
        name="prepare",
    )(index, latent, rope_key, query_wide, query_narrow, cosine, sine)


def attend_kernel(count, first, last, scales, *refs):
    fetched = 6 + count + (0 if first else 1)
    outs = refs[fetched : fetched + (2 if last else 1)]
    q, key_wide, value_wide, key_narrow, value_narrow, joined, old, keys, values, sems = refs[-10:]
    rows = q.shape[0] // 2
    width = key_wide.shape[0]
    targets = [q.at[:rows], q.at[rows:], key_wide, value_wide, key_narrow, value_narrow]
    begin = 0
    for piece in refs[6 : 6 + count]:
        targets.append(joined.at[begin : begin + piece.shape[0], :])
        begin += piece.shape[0]
    if not first:
        targets.append(old)
    fetch(refs[:fetched], targets, sems)
    latent = joined[:, :width]
    turned = joined[:, width:]
    wide_keys = dot_nn(latent, key_wide[...]).astype(BF16)
    narrow_keys = dot_nn(latent, key_narrow[...]).astype(BF16)
    lane = lax.broadcasted_iota(jnp.int32, narrow_keys.shape, 1)
    keys[:, 0:128] = wide_keys[:, :128]
    keys[:, 128:256] = turned
    keys[:, 256:384] = wide_keys[:, 128:]
    keys[:, 384:512] = turned
    keys[:, 512:640] = jnp.where(lane < NOPE_N, narrow_keys, turned)
    keys[:, 640:768] = jnp.where(lane < NOPE_N, turned, narrow_keys)
    values[:, :256] = dot_nn(latent, value_wide[...]).astype(BF16)
    values[:, 256:] = dot_nn(latent, value_narrow[...]).astype(BF16)
    spans = [(0, 256), (256, 512), (512, 640), (640, 768)]
    out_lane = lax.broadcasted_iota(jnp.int32, (2 * rows, 128), 1)

    def put(begin, end, value):
        if last:
            outs[0][:, begin:end] = value[:rows]
            outs[1][:, begin:end] = value[rows:]
        else:
            outs[0][:, begin:end] = value

    stats = jnp.zeros((2 * rows, 128), F32)
    narrow_parts = []
    for h in range(4):
        begin, end = spans[h]
        place = min(h, 2) * 128
        factor = scales[h] * LOG2E
        scores = dot_nt(q[:, begin:end], keys[:, begin:end])
        top = jnp.max(scores, axis=1, keepdims=True)
        if not first:
            old_top = old[:, 384 + h : 385 + h]
            old_sum = old[:, 388 + h : 389 + h]
            top = jnp.maximum(top, old_top)
            shrink = jnp.exp2((old_top - top) * factor)
        prob = jnp.exp2((scores - top) * factor)
        total = jnp.sum(prob, axis=1, keepdims=True)
        mixed = dot_nn(prob.astype(BF16), values[:, place : place + 128])
        if not first:
            total = total + old_sum * shrink
            mixed = mixed + old[:, place : place + 128] * shrink
        stats = jnp.where(out_lane == h, top, stats)
        stats = jnp.where(out_lane == 4 + h, total, stats)
        if h < 2:
            put(place, place + 128, mixed)
        else:
            narrow_parts.append(mixed)
    put(256, 384, jnp.where(out_lane < NOPE_N, narrow_parts[0], narrow_parts[1]))
    put(384, 512, stats)


def attend(queries, weights, pieces, state, scales, last=False):
    rows = queries[0].shape[0]
    keys = sum(p.shape[0] for p in pieces)
    first = state is None
    operands = [*queries, *weights, *pieces, *(() if first else (state,))]
    side = jax.ShapeDtypeStruct((rows, 512), F32)
    both = jax.ShapeDtypeStruct((2 * rows, 512), F32)
    return pl.pallas_call(
        functools.partial(attend_kernel, len(pieces), first, last, scales),
        out_shape=(side, side) if last else both,
        in_specs=[ANY] * len(operands),
        out_specs=(VMEM, VMEM) if last else VMEM,
        scratch_shapes=[
            pltpu.VMEM((2 * rows, 768), BF16),
            *(pltpu.VMEM(w.shape, BF16) for w in weights),
            pltpu.VMEM((keys, pieces[0].shape[1]), BF16),
            pltpu.VMEM((2 * rows, 512), F32),
            pltpu.VMEM((keys, 768), BF16),
            pltpu.VMEM((keys, 384), BF16),
            pltpu.SemaphoreType.DMA((len(operands),)),
        ],
        cost_estimate=pl.CostEstimate(
            flops=2 * keys * (512 * 768 + 2 * rows * 1280),
            bytes_accessed=8 * rows * 512 + 2 * keys * 640 + 2 * 512 * 768,
            transcendentals=8 * rows * keys,
        ),
        name="attend",
    )(*operands)


def project_kernel(parts, scales, index, *refs):
    outs = refs[4 : 4 + parts]
    mine, theirs, out_wide, out_narrow, scratch, sems = refs[4 + parts :]
    fetch(refs[:4], (mine, theirs, out_wide, out_narrow), sems)
    rows = mine.shape[0]
    lane = lax.broadcasted_iota(jnp.int32, (rows, 128), 1)
    pieces = []
    for h in range(4):
        factor = scales[h] * LOG2E
        top_a, top_b = mine[:, 384 + h : 385 + h], theirs[:, 384 + h : 385 + h]
        sum_a, sum_b = mine[:, 388 + h : 389 + h], theirs[:, 388 + h : 389 + h]
        top = jnp.maximum(top_a, top_b)
        shrink_a = jnp.exp2((top_a - top) * factor)
        shrink_b = jnp.exp2((top_b - top) * factor)
        total = sum_a * shrink_a + sum_b * shrink_b
        place = min(h, 2) * 128
        mixed = mine[:, place : place + 128] * shrink_a + theirs[:, place : place + 128] * shrink_b
        pieces.append(mixed / total)
    narrow = jnp.where(lane < NOPE_N, pieces[2], pieces[3])
    wide = jnp.concatenate(pieces[:2], axis=1).astype(BF16)
    scratch[...] = dot_nn(wide, out_wide[...]) + dot_nn(narrow.astype(BF16), out_narrow[...])
    share = rows // parts
    for d in range(parts):
        block = lax.rem(index[0] + d, parts)
        start = pl.multiple_of(block * share, 16)
        outs[d][...] = scratch[pl.ds(start, share), :].astype(BF16)


def project(index, mine, theirs, out_wide, out_narrow, parts, scales):
    rows, width = mine.shape[0], out_wide.shape[1]
    shape = jax.ShapeDtypeStruct((rows // parts, width), BF16)
    return pl.pallas_call(
        functools.partial(project_kernel, parts, scales),
        out_shape=(shape,) * parts,
        in_specs=[SMEM] + [ANY] * 4,
        out_specs=(VMEM,) * parts,
        scratch_shapes=[
            pltpu.VMEM(mine.shape, F32),
            pltpu.VMEM(theirs.shape, F32),
            pltpu.VMEM(out_wide.shape, BF16),
            pltpu.VMEM(out_narrow.shape, BF16),
            pltpu.VMEM((rows, width), F32),
            pltpu.SemaphoreType.DMA((4,)),
        ],
        cost_estimate=pl.CostEstimate(
            flops=2 * rows * width * 384, bytes_accessed=4 * rows * width, transcendentals=0
        ),
        name="project",
    )(index, mine, theirs, out_wide, out_narrow)


def mixer_kernel(parts, cuts, out_step, index, taps, before, after, *refs):
    blocks, weights = refs[:parts], refs[parts]
    outs = refs[parts + 1 : 2 * parts + 1]
    x, w_gate, w_value, w_down, gate, hidden, terms, sems = refs[2 * parts + 1 :]
    width, units = w_gate.shape
    at_tp = index[0]
    chunks = list(zip(cuts, cuts[1:]))
    copies = []
    for n, (begin, end) in enumerate(chunks):
        for which, target in enumerate((w_gate, w_value)):
            source = weights.at[:, which * units + begin : which * units + end]
            copies.append(
                pltpu.make_async_copy(source, target.at[:, begin:end], sems.at[which, n])
            )
    out_cuts = list(range(0, width, out_step))
    for n, begin in enumerate(out_cuts):
        source = weights.at[begin : begin + out_step, 2 * units :]
        copies.append(
            pltpu.make_async_copy(source, w_down.at[begin : begin + out_step, :], sems.at[2, n])
        )
    share = blocks[0].shape[0]
    rows = parts * share
    inputs = [
        pltpu.make_async_copy(before, x.at[:HALO, :], sems.at[3, 0]),
        pltpu.make_async_copy(after, x.at[HALO + rows :, :], sems.at[3, 1]),
    ]
    for d in range(parts):
        block = lax.rem(at_tp - d + parts, parts)
        start = pl.multiple_of(HALO + block * share, 16)
        inputs.append(
            pltpu.make_async_copy(blocks[d], x.at[pl.ds(start, share), :], sems.at[3, 2 + d])
        )
    for copy in inputs + copies:
        copy.start()
    for copy in inputs:
        copy.wait()
    for n, (begin, end) in enumerate(chunks):
        copies[2 * n].wait()
        gate[:, : end - begin] = dot_nn(x[...], w_gate[:, begin:end]).astype(BF16).astype(F32)
        copies[2 * n + 1].wait()
        value = dot_nn(x[HALO : HALO + rows, :], w_value[:, begin:end])
        mixed = jnp.zeros_like(value)
        for tap in range(taps.shape[0]):
            first = HALO - 1 + tap
            mixed = mixed + taps[tap : tap + 1, begin:end] * gate[first : first + rows, : end - begin]
        hidden[:, begin:end] = (mixed / (1.0 + jnp.exp(-mixed)) * value).astype(BF16)
    for n, begin in enumerate(out_cuts):
        copies[2 * len(chunks) + n].wait()
        terms[:, begin : begin + out_step] = dot_nt(hidden[...], w_down[begin : begin + out_step, :])
    for d in range(parts):
        block = lax.rem(at_tp + d, parts)
        start = pl.multiple_of(block * share, 16)
        outs[d][...] = terms[pl.ds(start, share), :].astype(BF16)


def mixer(index, taps, before, after, blocks, weights):
    parts = len(blocks)
    share, width = blocks[0].shape
    rows = parts * share
    units = weights.shape[1] // 3
    cuts = tuple(range(0, units, 384)) + (units,)
    out_step = width // 4
    return pl.pallas_call(
        functools.partial(mixer_kernel, parts, cuts, out_step),
        out_shape=(jax.ShapeDtypeStruct((share, width), BF16),) * parts,
        in_specs=[SMEM, VMEM] + [ANY] * (3 + parts),
        out_specs=(VMEM,) * parts,
        scratch_shapes=[
            pltpu.VMEM((2 * HALO + rows, width), BF16),
            pltpu.VMEM((width, units), BF16),
            pltpu.VMEM((width, units), BF16),
            pltpu.VMEM((width, units), BF16),
            pltpu.VMEM((2 * HALO + rows, 384), F32),
            pltpu.VMEM((rows, units), BF16),
            pltpu.VMEM((rows, width), F32),
            pltpu.SemaphoreType.DMA((4, max(len(cuts) - 1, 4, 2 + parts))),
        ],
        cost_estimate=pl.CostEstimate(
            flops=6 * rows * width * units,
            bytes_accessed=6 * width * units,
            transcendentals=rows * units,
        ),
        name="mixer",
    )(index, taps, before, after, *blocks, weights)


def fence(live):
    names = list(live)
    return dict(zip(names, lax.optimization_barrier(tuple(live[n] for n in names))))


def on_device(
    layer_input,
    latent,
    rope_key,
    query_wide,
    query_narrow,
    key_up_wide,
    value_up_wide,
    key_up_narrow,
    value_up_narrow,
    out_wide,
    out_narrow,
    norm_gain,
    gate_weight,
    value_weight,
    conv_weight,
    down_weight,
):
    n_sp, n_tp = lax.axis_size("sp"), lax.axis_size("tp")
    n_z = n_sp // CORES
    steps = {"up": n_z // 2, "down": n_z - 1 - n_z // 2}
    at_sp, at_tp = lax.axis_index("sp"), lax.axis_index("tp")
    index = at_tp.astype(jnp.int32)[None]
    z_moves = {"up": shift_perm(n_sp, CORES), "down": shift_perm(n_sp, -CORES)}
    x_moves = {"up": shift_perm(n_tp, 1), "down": shift_perm(n_tp, -1)}
    swap = partner_perm(n_sp)
    rows = latent.shape[0]
    rot = rope_key.shape[1]
    wide_scale = 1.0 / math.sqrt(NOPE_W + rot)
    narrow_scale = 1.0 / math.sqrt(NOPE_N + rot)
    scales = (wide_scale, wide_scale, narrow_scale, narrow_scale)
    up_weights = (key_up_wide, value_up_wide, key_up_narrow, value_up_narrow)

    stacked = jnp.concatenate([gate_weight, value_weight, down_weight.T], axis=1)
    weights = None

    cosine, sine = rope_tables(at_sp * rows, rows, rot)
    packed, half, q_own = prepare(
        index, latent, rope_key, query_wide, query_narrow, cosine, sine
    )
    live = {"up": half, "down": half, "q": q_own, "stacked": stacked}
    arrived, held = [packed], {"up": [], "down": []}
    state = None
    last = steps["up"]
    batch_ticks = (last // 2 + 1, last + 1)
    for tick in range(1, last + 2):
        new = {}
        if tick in batch_ticks:
            for way in ("up", "down"):
                pieces = [live[n] for n in held[way]]
                if not pieces:
                    continue
                joined = pieces[0] if len(pieces) == 1 else jnp.concatenate(pieces, axis=0)
                new["x" + way] = lax.ppermute(joined, "tp", x_moves[way])
        for way in ("up", "down"):
            if tick <= steps[way]:
                new[way] = lax.ppermute(live[way], "sp", z_moves[way])
        if tick == 1:
            new["q_other"] = lax.ppermute(live["q"], "sp", swap)
        if tick in batch_ticks:
            queries = (live["q"], live["q_other"])
            new["state"] = attend(queries, up_weights, arrived, state, scales)
            arrived, held = [], {"up": [], "down": []}
        for name in live:
            kept = name in ("q", "q_other", "stacked") or name in held["up"] + held["down"]
            if name not in new and kept:
                new[name] = live[name]
        live = fence(new)
        if tick == GATHER_AFTER:
            weights = lax.all_gather(live.pop("stacked"), "sp", axis=0, tiled=True)
        state = live.get("state", state)
        for way in ("up", "down"):
            if tick <= steps[way]:
                arrived.append(live[way])
                held[way].append(f"{way}{tick}")
                live[f"{way}{tick}"] = live[way]
            if "x" + way in live:
                arrived.append(live["x" + way])
    queries = (live["q"], live["q_other"])
    state = attend(queries, up_weights, arrived, state, scales, last=True)
    theirs = lax.ppermute(state[1], "sp", swap)
    blocks = project(index, state[0], theirs, out_wide, out_narrow, n_tp, scales)

    total = blocks[0].astype(F32)
    for d in range(1, n_tp):
        total = total + lax.ppermute(blocks[d], "tp", shift_perm(n_tp, d)).astype(F32)
    middle = (layer_input.astype(F32) + total).astype(BF16)
    full = middle.astype(F32)
    scale = lax.rsqrt(jnp.mean(full * full, axis=-1, keepdims=True) + norm_eps)
    normed = (full * scale * norm_gain).astype(BF16)
    blocks = [normed] + [
        lax.ppermute(normed, "tp", shift_perm(n_tp, d)) for d in range(1, n_tp)
    ]
    tails = jnp.stack([b[-HALO:] for b in blocks])
    heads = jnp.stack([b[:HALO] for b in blocks])
    tail = lax.dynamic_index_in_dim(tails, (at_tp + 1) % n_tp, 0, False)
    head = lax.dynamic_index_in_dim(heads, at_tp, 0, False)
    odd = at_sp % CORES == 1
    outward = [(i, i + 1) for i in range(1, n_sp - 1, CORES)]
    outward = outward + [(j, i) for i, j in outward]
    across = lax.ppermute(jnp.where(odd, tail, head), "sp", outward)
    within = lax.ppermute(jnp.where(odd, head, tail), "sp", swap)
    before = jnp.where(odd, within, across)
    after = jnp.where(odd, across, within)
    blocks, before, after, weights = lax.optimization_barrier((blocks, before, after, weights))
    terms = mixer(index, conv_weight, before, after, blocks, weights)
    total = terms[0].astype(F32)
    for d in range(1, n_tp):
        total = total + lax.ppermute(terms[d], "tp", shift_perm(n_tp, d)).astype(F32)
    return (middle.astype(F32) + total).astype(BF16)


def solution(mesh):
    in_specs = (
        P(("grp", "sp", "tp"), None),
        P(("grp", "sp"), None),
        P(("grp", "sp"), None),
        P(("grp", "sp"), "tp"),
        P(("grp", "sp"), "tp"),
        P(None, "tp"),
        P(None, "tp"),
        P(None, "tp"),
        P(None, "tp"),
        P("tp", None),
        P("tp", None),
        P(),
        P("sp", "tp"),
        P("sp", "tp"),
        P(None, "tp"),
        P("tp", "sp"),
    )
    out_specs = P(("grp", "sp", "tp"), None)
    return jax.shard_map(
        on_device, mesh=mesh, in_specs=in_specs, out_specs=out_specs, check_vma=False
    )
```

```python
import functools
import math

import jax
import jax.numpy as jnp
from jax import lax
from jax.experimental import pallas as pl
from jax.experimental.pallas import tpu as pltpu
from jax.sharding import PartitionSpec as P

NOPE_W = 128
NOPE_N = 64
CORES = 2
HALO = 16
GATHER_AFTER = 2
LOG2E = math.log2(math.e)

rope_base = 10000.0
norm_eps = 1e-06


F32 = jnp.float32
BF16 = jnp.bfloat16
VMEM = pl.BlockSpec(memory_space=pltpu.VMEM)
SMEM = pl.BlockSpec(memory_space=pltpu.SMEM)
ANY = pl.BlockSpec(memory_space=pl.ANY)


def shift_perm(size, by):
    return [(i, (i + by) % size) for i in range(size)]


def partner_perm(size):
    return [(i, i ^ 1) for i in range(size)]


def fetch(sources, targets, sems):
    copies = [
        pltpu.make_async_copy(source, target, sems.at[i])
        for i, (source, target) in enumerate(zip(sources, targets))
    ]
    for copy in copies:
        copy.start()
    for copy in copies:
        copy.wait()


def dot_nt(a, b):
    return lax.dot_general(a, b, (((1,), (1,)), ((), ())), preferred_element_type=F32)


def dot_nn(a, b):
    return jnp.dot(a, b, preferred_element_type=F32)


def rope_tables(row_start, row_total, span_width):
    places = (row_start + jnp.arange(row_total, dtype=jnp.int32)).astype(F32)
    frequency = jnp.power(
        rope_base, -jnp.arange(0, span_width, 2, dtype=jnp.int32).astype(F32) / span_width
    )
    angles = places[:, None] * frequency[None, :]
    angles = jnp.concatenate([angles, angles], axis=-1)
    return (jnp.cos(angles), jnp.sin(angles))


def prepare_kernel(
    index, latent, rope_key, query_wide, query_narrow, cosine, sine, packed, half, queries
):
    cos, sin = cosine[...], sine[...]
    rot = cos.shape[1]

    def spun(entries):
        entries = entries.astype(F32)
        half = rot // 2
        turned = jnp.concatenate([-entries[:, half:], entries[:, :half]], axis=1)
        return (entries * cos + turned * sin).astype(BF16)

    key = spun(rope_key[...])
    width = latent.shape[1]
    packed[:, :width] = latent[...]
    packed[:, width:] = jnp.concatenate([key, key], axis=1)
    share = half.shape[0]
    half[...] = packed[pl.ds(pl.multiple_of(lax.rem(index[0], 2) * share, 16), share), :]
    blank = jnp.zeros((cos.shape[0], rot), BF16)
    wide = query_wide[...]
    narrow = query_narrow[...]
    size = NOPE_W + rot
    for h in range(2):
        head = wide[:, h * size : (h + 1) * size]
        queries[:, 256 * h : 256 * h + NOPE_W] = head[:, :NOPE_W]
        queries[:, 256 * h + NOPE_W : 256 * h + 256] = jnp.concatenate(
            [spun(head[:, NOPE_W:]), blank], axis=1
        )
    size = NOPE_N + rot
    first, second = narrow[:, :size], narrow[:, size:]
    queries[:, 512:640] = jnp.concatenate([first[:, :NOPE_N], spun(first[:, NOPE_N:])], axis=1)
    queries[:, 640:768] = jnp.concatenate([spun(second[:, NOPE_N:]), second[:, :NOPE_N]], axis=1)


def prepare(index, latent, rope_key, query_wide, query_narrow, cosine, sine):
    rows = latent.shape[0]
    return pl.pallas_call(
        prepare_kernel,
        out_shape=(
            jax.ShapeDtypeStruct((rows, latent.shape[1] + 128), BF16),
            jax.ShapeDtypeStruct((rows // 2, latent.shape[1] + 128), BF16),
            jax.ShapeDtypeStruct((rows, 768), BF16),
        ),
        in_specs=[SMEM] + [VMEM] * 6,
        out_specs=(VMEM,) * 3,
        name="prepare",
    )(index, latent, rope_key, query_wide, query_narrow, cosine, sine)


def attend_kernel(count, first, last, scales, *refs):
    fetched = 6 + count + (0 if first else 1)
    outs = refs[fetched : fetched + (2 if last else 1)]
    q, key_wide, value_wide, key_narrow, value_narrow, joined, old, keys, values, sems = refs[-10:]
    rows = q.shape[0] // 2
    width = key_wide.shape[0]
    targets = [q.at[:rows], q.at[rows:], key_wide, value_wide, key_narrow, value_narrow]
    begin = 0
    for piece in refs[6 : 6 + count]:
        targets.append(joined.at[begin : begin + piece.shape[0], :])
        begin += piece.shape[0]
    if not first:
        targets.append(old)
    fetch(refs[:fetched], targets, sems)
    latent = joined[:, :width]
    turned = joined[:, width:]
    wide_keys = dot_nn(latent, key_wide[...]).astype(BF16)
    narrow_keys = dot_nn(latent, key_narrow[...]).astype(BF16)
    lane = lax.broadcasted_iota(jnp.int32, narrow_keys.shape, 1)
    keys[:, 0:128] = wide_keys[:, :128]
    keys[:, 128:256] = turned
    keys[:, 256:384] = wide_keys[:, 128:]
    keys[:, 384:512] = turned
    keys[:, 512:640] = jnp.where(lane < NOPE_N, narrow_keys, turned)
    keys[:, 640:768] = jnp.where(lane < NOPE_N, turned, narrow_keys)
    values[:, :256] = dot_nn(latent, value_wide[...]).astype(BF16)
    values[:, 256:] = dot_nn(latent, value_narrow[...]).astype(BF16)
    spans = [(0, 256), (256, 512), (512, 640), (640, 768)]
    out_lane = lax.broadcasted_iota(jnp.int32, (2 * rows, 128), 1)

    def put(begin, end, value):
        if last:
            outs[0][:, begin:end] = value[:rows]
            outs[1][:, begin:end] = value[rows:]
        else:
            outs[0][:, begin:end] = value

    stats = jnp.zeros((2 * rows, 128), F32)
    narrow_parts = []
    for h in range(4):
        begin, end = spans[h]
        place = min(h, 2) * 128
        factor = scales[h] * LOG2E
        scores = dot_nt(q[:, begin:end], keys[:, begin:end])
        top = jnp.max(scores, axis=1, keepdims=True)
        if not first:
            old_top = old[:, 384 + h : 385 + h]
            old_sum = old[:, 388 + h : 389 + h]
            top = jnp.maximum(top, old_top)
            shrink = jnp.exp2((old_top - top) * factor)
        prob = jnp.exp2((scores - top) * factor)
        total = jnp.sum(prob, axis=1, keepdims=True)
        mixed = dot_nn(prob.astype(BF16), values[:, place : place + 128])
        if not first:
            total = total + old_sum * shrink
            mixed = mixed + old[:, place : place + 128] * shrink
        stats = jnp.where(out_lane == h, top, stats)
        stats = jnp.where(out_lane == 4 + h, total, stats)
        if h < 2:
            put(place, place + 128, mixed)
        else:
            narrow_parts.append(mixed)
    put(256, 384, jnp.where(out_lane < NOPE_N, narrow_parts[0], narrow_parts[1]))
    put(384, 512, stats)


def attend(queries, weights, pieces, state, scales, last=False):
    rows = queries[0].shape[0]
    keys = sum(p.shape[0] for p in pieces)
    first = state is None
    operands = [*queries, *weights, *pieces, *(() if first else (state,))]
    side = jax.ShapeDtypeStruct((rows, 512), F32)
    both = jax.ShapeDtypeStruct((2 * rows, 512), F32)
    return pl.pallas_call(
        functools.partial(attend_kernel, len(pieces), first, last, scales),
        out_shape=(side, side) if last else both,
        in_specs=[ANY] * len(operands),
        out_specs=(VMEM, VMEM) if last else VMEM,
        scratch_shapes=[
            pltpu.VMEM((2 * rows, 768), BF16),
            *(pltpu.VMEM(w.shape, BF16) for w in weights),
            pltpu.VMEM((keys, pieces[0].shape[1]), BF16),
            pltpu.VMEM((2 * rows, 512), F32),
            pltpu.VMEM((keys, 768), BF16),
            pltpu.VMEM((keys, 384), BF16),
            pltpu.SemaphoreType.DMA((len(operands),)),
        ],
        cost_estimate=pl.CostEstimate(
            flops=2 * keys * (512 * 768 + 2 * rows * 1280),
            bytes_accessed=8 * rows * 512 + 2 * keys * 640 + 2 * 512 * 768,
            transcendentals=8 * rows * keys,
        ),
        name="attend",
    )(*operands)


def project_kernel(parts, scales, index, *refs):
    outs = refs[4 : 4 + parts]
    mine, theirs, out_wide, out_narrow, scratch, sems = refs[4 + parts :]
    fetch(refs[:4], (mine, theirs, out_wide, out_narrow), sems)
    rows = mine.shape[0]
    lane = lax.broadcasted_iota(jnp.int32, (rows, 128), 1)
    pieces = []
    for h in range(4):
        factor = scales[h] * LOG2E
        top_a, top_b = mine[:, 384 + h : 385 + h], theirs[:, 384 + h : 385 + h]
        sum_a, sum_b = mine[:, 388 + h : 389 + h], theirs[:, 388 + h : 389 + h]
        top = jnp.maximum(top_a, top_b)
        shrink_a = jnp.exp2((top_a - top) * factor)
        shrink_b = jnp.exp2((top_b - top) * factor)
        total = sum_a * shrink_a + sum_b * shrink_b
        place = min(h, 2) * 128
        mixed = mine[:, place : place + 128] * shrink_a + theirs[:, place : place + 128] * shrink_b
        pieces.append(mixed / total)
    narrow = jnp.where(lane < NOPE_N, pieces[2], pieces[3])
    wide = jnp.concatenate(pieces[:2], axis=1).astype(BF16)
    scratch[...] = dot_nn(wide, out_wide[...]) + dot_nn(narrow.astype(BF16), out_narrow[...])
    share = rows // parts
    for d in range(parts):
        block = lax.rem(index[0] + d, parts)
        start = pl.multiple_of(block * share, 16)
        outs[d][...] = scratch[pl.ds(start, share), :].astype(BF16)


def project(index, mine, theirs, out_wide, out_narrow, parts, scales):
    rows, width = mine.shape[0], out_wide.shape[1]
    shape = jax.ShapeDtypeStruct((rows // parts, width), BF16)
    return pl.pallas_call(
        functools.partial(project_kernel, parts, scales),
        out_shape=(shape,) * parts,
        in_specs=[SMEM] + [ANY] * 4,
        out_specs=(VMEM,) * parts,
        scratch_shapes=[
            pltpu.VMEM(mine.shape, F32),
            pltpu.VMEM(theirs.shape, F32),
            pltpu.VMEM(out_wide.shape, BF16),
            pltpu.VMEM(out_narrow.shape, BF16),
            pltpu.VMEM((rows, width), F32),
            pltpu.SemaphoreType.DMA((4,)),
        ],
        cost_estimate=pl.CostEstimate(
            flops=2 * rows * width * 384, bytes_accessed=4 * rows * width, transcendentals=0
        ),
        name="project",
    )(index, mine, theirs, out_wide, out_narrow)


def mixer_kernel(parts, cuts, out_step, index, taps, before, after, *refs):
    blocks, weights = refs[:parts], refs[parts]
    outs = refs[parts + 1 : 2 * parts + 1]
    x, w_gate, w_value, w_down, gate, hidden, terms, sems = refs[2 * parts + 1 :]
    width, units = w_gate.shape
    at_tp = index[0]
    chunks = list(zip(cuts, cuts[1:]))
    copies = []
    for n, (begin, end) in enumerate(chunks):
        for which, target in enumerate((w_gate, w_value)):
            source = weights.at[:, which * units + begin : which * units + end]
            copies.append(
                pltpu.make_async_copy(source, target.at[:, begin:end], sems.at[which, n])
            )
    out_cuts = list(range(0, width, out_step))
    for n, begin in enumerate(out_cuts):
        source = weights.at[begin : begin + out_step, 2 * units :]
        copies.append(
            pltpu.make_async_copy(source, w_down.at[begin : begin + out_step, :], sems.at[2, n])
        )
    share = blocks[0].shape[0]
    rows = parts * share
    inputs = [
        pltpu.make_async_copy(before, x.at[:HALO, :], sems.at[3, 0]),
        pltpu.make_async_copy(after, x.at[HALO + rows :, :], sems.at[3, 1]),
    ]
    for d in range(parts):
        block = lax.rem(at_tp - d + parts, parts)
        start = pl.multiple_of(HALO + block * share, 16)
        inputs.append(
            pltpu.make_async_copy(blocks[d], x.at[pl.ds(start, share), :], sems.at[3, 2 + d])
        )
    for copy in inputs + copies:
        copy.start()
    for copy in inputs:
        copy.wait()
    for n, (begin, end) in enumerate(chunks):
        copies[2 * n].wait()
        gate[:, : end - begin] = dot_nn(x[...], w_gate[:, begin:end]).astype(BF16).astype(F32)
        copies[2 * n + 1].wait()
        value = dot_nn(x[HALO : HALO + rows, :], w_value[:, begin:end])
        mixed = jnp.zeros_like(value)
        for tap in range(taps.shape[0]):
            first = HALO - 1 + tap
            mixed = mixed + taps[tap : tap + 1, begin:end] * gate[first : first + rows, : end - begin]
        hidden[:, begin:end] = (mixed / (1.0 + jnp.exp(-mixed)) * value).astype(BF16)

    def project_down(n, carry):
        span = pl.ds(pl.multiple_of(n * out_step, 128), out_step)
        source = weights.at[span, 2 * units :]
        pltpu.make_async_copy(source, w_down.at[span, :], sems.at[2, n]).wait()
        terms[:, span] = dot_nt(hidden[...], w_down[span, :])
        return carry

    lax.fori_loop(0, len(out_cuts), project_down, 0)
    for d in range(parts):
        block = lax.rem(at_tp + d, parts)
        start = pl.multiple_of(block * share, 16)
        outs[d][...] = terms[pl.ds(start, share), :].astype(BF16)


def mixer(index, taps, before, after, blocks, weights):
    parts = len(blocks)
    share, width = blocks[0].shape
    rows = parts * share
    units = weights.shape[1] // 3
    cuts = tuple(range(0, units, 384)) + (units,)
    out_step = width // 4
    return pl.pallas_call(
        functools.partial(mixer_kernel, parts, cuts, out_step),
        out_shape=(jax.ShapeDtypeStruct((share, width), BF16),) * parts,
        in_specs=[SMEM, VMEM] + [ANY] * (3 + parts),
        out_specs=(VMEM,) * parts,
        scratch_shapes=[
            pltpu.VMEM((2 * HALO + rows, width), BF16),
            pltpu.VMEM((width, units), BF16),
            pltpu.VMEM((width, units), BF16),
            pltpu.VMEM((width, units), BF16),
            pltpu.VMEM((2 * HALO + rows, 384), F32),
            pltpu.VMEM((rows, units), BF16),
            pltpu.VMEM((rows, width), F32),
            pltpu.SemaphoreType.DMA((4, max(len(cuts) - 1, 4, 2 + parts))),
        ],
        cost_estimate=pl.CostEstimate(
            flops=6 * rows * width * units,
            bytes_accessed=6 * width * units,
            transcendentals=rows * units,
        ),
        name="mixer",
    )(index, taps, before, after, *blocks, weights)


def fence(live):
    names = list(live)
    return dict(zip(names, lax.optimization_barrier(tuple(live[n] for n in names))))


def on_device(
    layer_input,
    latent,
    rope_key,
    query_wide,
    query_narrow,
    key_up_wide,
    value_up_wide,
    key_up_narrow,
    value_up_narrow,
    out_wide,
    out_narrow,
    norm_gain,
    gate_weight,
    value_weight,
    conv_weight,
    down_weight,
):
    n_sp, n_tp = lax.axis_size("sp"), lax.axis_size("tp")
    n_z = n_sp // CORES
    steps = {"up": n_z // 2, "down": n_z - 1 - n_z // 2}
    at_sp, at_tp = lax.axis_index("sp"), lax.axis_index("tp")
    index = at_tp.astype(jnp.int32)[None]
    z_moves = {"up": shift_perm(n_sp, CORES), "down": shift_perm(n_sp, -CORES)}
    x_moves = {"up": shift_perm(n_tp, 1), "down": shift_perm(n_tp, -1)}
    swap = partner_perm(n_sp)
    rows = latent.shape[0]
    rot = rope_key.shape[1]
    wide_scale = 1.0 / math.sqrt(NOPE_W + rot)
    narrow_scale = 1.0 / math.sqrt(NOPE_N + rot)
    scales = (wide_scale, wide_scale, narrow_scale, narrow_scale)
    up_weights = (key_up_wide, value_up_wide, key_up_narrow, value_up_narrow)

    stacked = jnp.concatenate([gate_weight, value_weight, down_weight.T], axis=1)
    weights = None

    cosine, sine = rope_tables(at_sp * rows, rows, rot)
    packed, half, q_own = prepare(
        index, latent, rope_key, query_wide, query_narrow, cosine, sine
    )
    live = {"up": half, "down": half, "q": q_own, "stacked": stacked}
    arrived, held = [packed], {"up": [], "down": []}
    state = None
    last = steps["up"]
    batch_ticks = (last // 2 + 1, last + 1)
    for tick in range(1, last + 2):
        new = {}
        if tick in batch_ticks:
            for way in ("up", "down"):
                pieces = [live[n] for n in held[way]]
                if not pieces:
                    continue
                joined = pieces[0] if len(pieces) == 1 else jnp.concatenate(pieces, axis=0)
                new["x" + way] = lax.ppermute(joined, "tp", x_moves[way])
        for way in ("up", "down"):
            if tick <= steps[way]:
                new[way] = lax.ppermute(live[way], "sp", z_moves[way])
        if tick == 1:
            new["q_other"] = lax.ppermute(live["q"], "sp", swap)
        if tick in batch_ticks:
            queries = (live["q"], live["q_other"])
            new["state"] = attend(queries, up_weights, arrived, state, scales)
            arrived, held = [], {"up": [], "down": []}
        for name in live:
            kept = name in ("q", "q_other", "stacked") or name in held["up"] + held["down"]
            if name not in new and kept:
                new[name] = live[name]
        live = fence(new)
        if tick == GATHER_AFTER:
            weights = lax.all_gather(live.pop("stacked"), "sp", axis=0, tiled=True)
        state = live.get("state", state)
        for way in ("up", "down"):
            if tick <= steps[way]:
                arrived.append(live[way])
                held[way].append(f"{way}{tick}")
                live[f"{way}{tick}"] = live[way]
            if "x" + way in live:
                arrived.append(live["x" + way])
    queries = (live["q"], live["q_other"])
    state = attend(queries, up_weights, arrived, state, scales, last=True)
    theirs = lax.ppermute(state[1], "sp", swap)
    blocks = project(index, state[0], theirs, out_wide, out_narrow, n_tp, scales)

    total = blocks[0].astype(F32)
    for d in range(1, n_tp):
        total = total + lax.ppermute(blocks[d], "tp", shift_perm(n_tp, d)).astype(F32)
    middle = (layer_input.astype(F32) + total).astype(BF16)
    full = middle.astype(F32)
    scale = lax.rsqrt(jnp.mean(full * full, axis=-1, keepdims=True) + norm_eps)
    normed = (full * scale * norm_gain).astype(BF16)
    blocks = [normed] + [
        lax.ppermute(normed, "tp", shift_perm(n_tp, d)) for d in range(1, n_tp)
    ]
    tails = jnp.stack([b[-HALO:] for b in blocks])
    heads = jnp.stack([b[:HALO] for b in blocks])
    tail = lax.dynamic_index_in_dim(tails, (at_tp + 1) % n_tp, 0, False)
    head = lax.dynamic_index_in_dim(heads, at_tp, 0, False)
    odd = at_sp % CORES == 1
    outward = [(i, i + 1) for i in range(1, n_sp - 1, CORES)]
    outward = outward + [(j, i) for i, j in outward]
    across = lax.ppermute(jnp.where(odd, tail, head), "sp", outward)
    within = lax.ppermute(jnp.where(odd, head, tail), "sp", swap)
    before = jnp.where(odd, within, across)
    after = jnp.where(odd, across, within)
    blocks, before, after, weights = lax.optimization_barrier((blocks, before, after, weights))
    terms = mixer(index, conv_weight, before, after, blocks, weights)
    total = terms[0].astype(F32)
    for d in range(1, n_tp):
        total = total + lax.ppermute(terms[d], "tp", shift_perm(n_tp, d)).astype(F32)
    return (middle.astype(F32) + total).astype(BF16)


def solution(mesh):
    in_specs = (
        P(("grp", "sp", "tp"), None),
        P(("grp", "sp"), None),
        P(("grp", "sp"), None),
        P(("grp", "sp"), "tp"),
        P(("grp", "sp"), "tp"),
        P(None, "tp"),
        P(None, "tp"),
        P(None, "tp"),
        P(None, "tp"),
        P("tp", None),
        P("tp", None),
        P(),
        P("sp", "tp"),
        P("sp", "tp"),
        P(None, "tp"),
        P("tp", "sp"),
    )
    out_specs = P(("grp", "sp", "tp"), None)
    return jax.shard_map(
        on_device, mesh=mesh, in_specs=in_specs, out_specs=out_specs, check_vma=False
    )
```
